32 devices in a mesh: sp: 8 (over z, x), tp: 4 (over y, core).
Axes of the slice: x: 2, y: 2, z: 4, core: 2. Of those that a mesh axis runs over, the one named last changes fastest.
Arguments:
- query_rows: bfloat16 [8192, 1024], P('sp', 'tp'), may hold values from -8 to 8
- key_rows: bfloat16 [8192, 1024], P('sp', 'tp'), may hold values from -8 to 8
- value_rows: bfloat16 [8192, 1024], P('sp', 'tp'), may hold values from -6 to 6
- forget_cum: float32 [16, 8192], P('tp', 'sp'), may hold values from -8192 to 0, as said below
- doc_ids: int32 [8192], P('sp'), may hold values from 0 to 3, never falling along the last dimension, each value on 1 to 3072 neighbouring positions
- residual: bfloat16 [8192, 2048], P(('sp', 'tp')), may hold values from -6 to 6
- out_weight: bfloat16 [1024, 2048], replicated, may hold values from -1.5 to 1.5
- norm_gain: float32 [2048], replicated, may hold values from 0.1 to 1.9
- expert_ids: int32 [8192, 2], P(('sp', 'tp')), may hold values from 0 to 7, as said below
- route_weights: float32 [8192, 2], P(('sp', 'tp')), may hold values from 0.2 to 1
- gate_proj: bfloat16 [8, 2048, 512], P('sp'), may hold values from -0.125 to 0.125
- up_proj: bfloat16 [8, 2048, 512], P('sp'), may hold values from -0.125 to 0.125
- down_proj: bfloat16 [8, 512, 2048], P('sp'), may hold values from -0.25 to 0.25
Outputs:
- layer_out: bfloat16 [8192, 2048], P(('sp', 'tp'))
The draws below stay inside these ranges and needn't reach their ends.
Inputs may be any that keep to these rules, and one draw needn't show every extreme that they name: `forget_cum`: each head's values never rise along the positions. `doc_ids`: document numbers never fall along the positions; a document holds at most 3072 positions, and one holds exactly 3072. `expert_ids`: a token's 2 experts differ and lie in one group of 4 consecutive experts; among the 256 rows of one device no expert is named more than 160 times, and in every draw one expert is named exactly 160 times by the rows of every device.
All inputs are finite; a program needn't handle non-finite values.
Results may differ from the reference program's by a relative error of at most 0.0054.
Values may be sent and summed in bfloat16 or wider, within the bound.
No kernel may reach another device: no remote copies, remote signals or barrier semaphores. Data moves between devices by JAX's collectives and lax.ppermute only.
A program may use at most 128 MiB of HBM per device.

```python
import math
import jax
import jax.numpy as jnp
import numpy as np
from jax import lax

D = 2048
HEAD_COUNT = 16
HD = 64
FFE = 512
EPG = 4
TOPK = 2
REACH = 3
TOK_DEV = 1024
TOKEN_COUNT = 8192
TOK_LOC = 256
MOST = 3072
DOCS = 4
EXPERTS = 8
GROUPS = 2
CAP = 160


def draw_query_rows(key, part):
    width = HEAD_COUNT * HD
    base = jnp.clip(jax.random.normal(jax.random.fold_in(key, 1), (TOKEN_COUNT, width), jnp.float32), -6.0, 6.0)
    return base.astype(jnp.bfloat16)


def draw_key_rows(key, part):
    width = HEAD_COUNT * HD
    base = jnp.clip(jax.random.normal(jax.random.fold_in(key, 3), (TOKEN_COUNT, width), jnp.float32), -6.0, 6.0)
    return base.astype(jnp.bfloat16)


def draw_forget_cum(key, part):
    order = jax.random.permutation(jax.random.fold_in(key, 5), HEAD_COUNT)
    fast_count = HEAD_COUNT // 2
    quick_route = order < fast_count
    fast_rate = jnp.exp(jax.random.uniform(jax.random.fold_in(key, 6), (HEAD_COUNT,), jnp.float32, jnp.log(1.0 / 100.0), jnp.log(1.0 / 30.0)))
    slow_rate = jnp.exp(jax.random.uniform(jax.random.fold_in(key, 7), (HEAD_COUNT,), jnp.float32, jnp.log(0.3), jnp.log(1.0))) / TOKEN_COUNT
    rate = jnp.where(quick_route, fast_rate, slow_rate)
    device_factor = jnp.exp(jax.random.uniform(jax.random.fold_in(key, 8), (HEAD_COUNT, TOKEN_COUNT // TOK_DEV), jnp.float32, jnp.log(0.5), jnp.log(2.0)))
    device_factor = jnp.repeat(device_factor, TOK_DEV, axis=1)
    rough = jax.random.uniform(jax.random.fold_in(key, 9), (HEAD_COUNT, TOKEN_COUNT), jnp.float32, 0.0, 2.0)
    gate_logarithm = -rate[:, None] * device_factor * rough
    spike_positions = jax.random.randint(jax.random.fold_in(key, 10), (HEAD_COUNT, 2), 0, TOKEN_COUNT)
    spike_loss = jax.random.uniform(jax.random.fold_in(key, 11), (HEAD_COUNT, 2), jnp.float32, jnp.log(0.5), jnp.log(0.8))
    target_locations = jnp.arange(TOKEN_COUNT, dtype=jnp.int32)
    match_counts = target_locations[None, None, :] == spike_positions[:, :, None]
    spike_events = jnp.sum(jnp.where(match_counts, spike_loss[:, :, None], 0.0), axis=1)
    gate_logarithm = gate_logarithm + jnp.where(quick_route[:, None], 0.0, spike_events)
    return jnp.cumsum(gate_logarithm, axis=1).astype(jnp.float32)


def draw_expert_ids(key, part):
    block_total = TOKEN_COUNT // TOK_LOC
    busy_group = jax.random.randint(jax.random.fold_in(key, 12), (), 0, GROUPS)
    busy_local = jax.random.randint(jax.random.fold_in(key, 13), (), 0, EPG)

    def one_block(block_key):
        others = jnp.arange((GROUPS - 1) * CAP, dtype=jnp.int32) // CAP
        others = others + (others >= busy_group).astype(jnp.int32)
        chosen = jax.random.permutation(jax.random.fold_in(block_key, 1), others)[:TOK_LOC - CAP]
        groups = jnp.concatenate([jnp.full((CAP,), busy_group, jnp.int32), chosen.astype(jnp.int32)])
        groups = jax.random.permutation(jax.random.fold_in(block_key, 2), groups)
        first = jax.random.randint(jax.random.fold_in(block_key, 3), (TOK_LOC,), 0, EPG)
        first = jnp.where(groups == busy_group, busy_local, first)
        second = (first + jax.random.randint(jax.random.fold_in(block_key, 4), (TOK_LOC,), 1, EPG)) % EPG
        swap = jax.random.randint(jax.random.fold_in(block_key, 5), (TOK_LOC,), 0, 2)
        lower = jnp.where(swap == 1, second, first)
        upper = jnp.where(swap == 1, first, second)
        return jnp.stack([groups * EPG + lower, groups * EPG + upper], axis=1).astype(jnp.int32)
    block_keys = jax.random.split(jax.random.fold_in(key, 14), block_total)
    return jax.vmap(one_block)(block_keys).reshape(TOKEN_COUNT, TOPK).astype(jnp.int32)


def shard_levels(stream_key, shape, cuts, least, largest):
    def one(position, blocks):
        draws = jax.random.uniform(jax.random.fold_in(jax.random.fold_in(stream_key, 6), position), (blocks,), jnp.float32, least / len(cuts), largest / len(cuts))
        return jnp.repeat(jnp.exp(draws), shape[position] // blocks).reshape((-1,) + (1,) * (len(shape) - position - 1))

    gain = one(*cuts[0])
    for cut in cuts[1:]:
        gain = gain * one(*cut)
    return gain


def split_up(amount, total, reach, slope):
    loads = [(1 << 20) // math.isqrt(standing ** slope) + 1 for standing in range(2, amount + 1)]
    rest, given = total - reach - (amount - 1), [1] * (amount - 1)
    while rest > 0:
        candidates = [i for i in range(amount - 1) if given[i] < reach]
        mass, left = sum([loads[i] for i in candidates]), rest
        for i in candidates:
            addition = min(reach - given[i], max(1, left * loads[i] // mass), rest)
            given[i] = given[i] + addition
            rest = rest - addition
    return np.array([reach] + given)


def ragged(key, count, total, limit, slope):
    if count == 2:
        one = jax.random.randint(key, (), max(1, total - limit), min(limit, total - 1) + 1)
        return jnp.stack([one, total - one])
    tallies = jnp.asarray(split_up(count, total, limit, slope), jnp.int32)
    pairs = (count - 1) // 2
    source_of, taker = tallies[1:1 + 2 * pairs:2], tallies[2:2 + 2 * pairs:2]
    slack = jnp.minimum(source_of - 1, limit - taker)
    moved = jax.random.randint(jax.random.fold_in(key, 1), (pairs,), 0, 1 << 20) % (slack + 1)
    tallies = tallies.at[1:1 + 2 * pairs:2].set(source_of - moved).at[2:2 + 2 * pairs:2].set(taker + moved)
    return tallies[jax.random.permutation(jax.random.fold_in(key, 2), count)]


def bell_draw(rng, shape, deviation, bound, pieces=(), kind=jnp.bfloat16):
    drawn = jax.random.normal(rng, shape, jnp.float32) * deviation
    if len(pieces) > 0:
        drawn = shard_levels(rng, shape, pieces, -0.22, 0.18) * drawn
    return jnp.clip(drawn, min=-bound, max=bound).astype(kind)


def setup_inputs(seed: int = 0) -> dict:
    key_of = jax.random.split(jax.random.key(seed), 14)
    query_rows = draw_query_rows(jax.random.fold_in(key_of[13], 71), 0)
    key_rows = draw_key_rows(jax.random.fold_in(key_of[13], 71), 0)
    value_rows = bell_draw(key_of[2], (TOKEN_COUNT, HEAD_COUNT * HD), 1.0, 6.0, ((0, 8), (1, 4)))
    forget_cum = draw_forget_cum(jax.random.fold_in(key_of[13], 71), 0)
    doc_ids = jnp.searchsorted(jnp.cumsum(ragged(key_of[4], DOCS, TOKEN_COUNT, MOST, 2)), jnp.arange(TOKEN_COUNT), side="right").astype(jnp.int32)
    residual = bell_draw(key_of[5], (TOKEN_COUNT, D), 1.0, 6.0, ((0, 32),))
    out_weight = bell_draw(key_of[6], (HEAD_COUNT * HD, D), HEAD_COUNT ** -0.5, 1.5)
    norm_gain = jnp.clip(1.0 + 0.18 * jax.random.normal(key_of[7], (D,), jnp.float32), 0.1, 1.9)
    expert_ids = draw_expert_ids(jax.random.fold_in(key_of[13], 71), 0)
    route_weights = jnp.clip(0.2 + 0.8 * jax.random.uniform(key_of[9], (TOKEN_COUNT, TOPK), jnp.float32) ** shard_levels(key_of[9], (TOKEN_COUNT, TOPK), ((0, 32),), -0.2, 0.2), 0.2, 1.0)
    gate_proj = bell_draw(key_of[10], (EXPERTS, D, FFE), D ** -0.5, 0.125, ((0, 8),))
    up_proj = bell_draw(key_of[11], (EXPERTS, D, FFE), D ** -0.5, 0.125, ((0, 8),))
    down_proj = bell_draw(key_of[12], (EXPERTS, FFE, D), FFE ** -0.5, 0.25, ((0, 8),))
    return dict(query_rows=query_rows, key_rows=key_rows, value_rows=value_rows, forget_cum=forget_cum, doc_ids=doc_ids, residual=residual, out_weight=out_weight, norm_gain=norm_gain, expert_ids=expert_ids, route_weights=route_weights, gate_proj=gate_proj, up_proj=up_proj, down_proj=down_proj)


norm_eps = 1e-06
row_block = 128

def attention(query_rows, key_rows, value_rows, forget_cum, doc_ids):
    width = HEAD_COUNT * HD
    back = REACH * TOK_DEV
    span = back + TOK_DEV
    keys_pad = jnp.concatenate([jnp.zeros((back, width), jnp.bfloat16), key_rows], axis=0)
    values_pad = jnp.concatenate([jnp.zeros((back, width), jnp.bfloat16), value_rows], axis=0)
    gates_pad = jnp.concatenate([jnp.zeros((HEAD_COUNT, back), jnp.float32), forget_cum], axis=1)
    docs_pad = jnp.concatenate([jnp.full((back,), -1, jnp.int32), doc_ids.astype(jnp.int32)], axis=0)
    scale = HD ** (-0.5)

    def attend_block(index):
        start = (index * TOK_DEV).astype(jnp.int32)
        query = lax.dynamic_slice_in_dim(query_rows, start, TOK_DEV, 0).reshape(TOK_DEV, HEAD_COUNT, HD).astype(jnp.float32)
        keys = lax.dynamic_slice_in_dim(keys_pad, start, span, 0).reshape(span, HEAD_COUNT, HD).astype(jnp.float32)
        values = lax.dynamic_slice_in_dim(values_pad, start, span, 0).reshape(span, HEAD_COUNT, HD).astype(jnp.float32)
        query_gate = lax.dynamic_slice_in_dim(forget_cum, start, TOK_DEV, 1)
        key_gate = lax.dynamic_slice_in_dim(gates_pad, start, span, 1)
        query_doc = lax.dynamic_slice_in_dim(doc_ids.astype(jnp.int32), start, TOK_DEV, 0)
        key_doc = lax.dynamic_slice_in_dim(docs_pad, start, span, 0)
        score = jnp.einsum('thd,uhd->htu', query, keys) * scale
        score = score + query_gate[:, :, None] - key_gate[:, None, :]
        query_pos = start + jnp.arange(TOK_DEV, dtype=jnp.int32)
        key_pos = start - back + jnp.arange(span, dtype=jnp.int32)
        allowed = (key_pos[None, :] <= query_pos[:, None]) & (key_doc[None, :] == query_doc[:, None])
        score = jnp.where(allowed[None], score, -jnp.inf)
        top = lax.optimization_barrier(jnp.max(score, axis=-1))
        expo = jnp.exp(score - top[..., None])
        total = lax.optimization_barrier(jnp.sum(expo, axis=-1))
        rounded = lax.optimization_barrier(expo.astype(jnp.bfloat16)).astype(jnp.float32)
        summed = jnp.einsum('htu,uhd->thd', rounded, values)
        result = summed / jnp.transpose(total)[:, :, None]
        return result.astype(jnp.bfloat16).reshape(TOK_DEV, width)
    blocks = lax.map(attend_block, jnp.arange(TOKEN_COUNT // TOK_DEV, dtype=jnp.int32))
    return blocks.reshape(TOKEN_COUNT, width)

def experts_layer(normed, expert_ids, route_weights, gate_proj, up_proj, down_proj):
    assign = TOKEN_COUNT * TOPK
    flat_expert = expert_ids.reshape(assign).astype(jnp.int32)
    flat_token = (jnp.arange(assign, dtype=jnp.int32) // TOPK).astype(jnp.int32)
    flat_weight = route_weights.reshape(assign)
    order = jnp.argsort(flat_expert, stable=True)
    sorted_expert = flat_expert[order]
    sorted_token = flat_token[order]
    sorted_weight = flat_weight[order]
    counts = jnp.bincount(flat_expert, length=EXPERTS).astype(jnp.int32)
    padded = (counts + row_block - 1) // row_block * row_block
    start = jnp.cumsum(counts) - counts
    pad_end = jnp.cumsum(padded)
    pad_start = pad_end - padded
    dest = (pad_start[sorted_expert] + jnp.arange(assign, dtype=jnp.int32) - start[sorted_expert]).astype(jnp.int32)
    block_count = (assign + EXPERTS * (row_block - 1) + row_block - 1) // row_block
    buffer = jnp.zeros((block_count * row_block, D), jnp.bfloat16).at[dest].set(normed[sorted_token])
    block_expert = jnp.clip(jnp.searchsorted(pad_end, jnp.arange(block_count, dtype=jnp.int32) * row_block, side='right'), 0, EXPERTS - 1).astype(jnp.int32)

    def run_block(args):
        rows, expert = args
        gate = jnp.dot(rows, gate_proj[expert], preferred_element_type=jnp.float32)
        up = jnp.dot(rows, up_proj[expert], preferred_element_type=jnp.float32)
        act = (jax.nn.silu(gate) * up).astype(jnp.bfloat16)
        return jnp.dot(act, down_proj[expert], preferred_element_type=jnp.float32).astype(jnp.bfloat16)
    results = lax.map(run_block, (buffer.reshape(block_count, row_block, D), block_expert)).reshape(-1, D)
    contrib = results[dest].astype(jnp.float32) * sorted_weight[:, None]
    return jnp.zeros((TOKEN_COUNT, D), jnp.float32).at[sorted_token].add(contrib)

def reference(query_rows, key_rows, value_rows, forget_cum, doc_ids, residual, out_weight, norm_gain, expert_ids, route_weights, gate_proj, up_proj, down_proj):
    attended = attention(query_rows, key_rows, value_rows, forget_cum, doc_ids)
    mixed = jnp.dot(attended, out_weight, preferred_element_type=jnp.float32)
    hidden = residual.astype(jnp.float32) + mixed
    normed = (hidden * lax.rsqrt(lax.optimization_barrier(jnp.mean(hidden * hidden, axis=-1, keepdims=True)) + norm_eps) * norm_gain).astype(jnp.bfloat16)
    routed = experts_layer(normed, expert_ids, route_weights, gate_proj, up_proj, down_proj)
    return (hidden + routed).astype(jnp.bfloat16)
```

```python
import functools

import jax
import jax.numpy as jnp
from jax import lax
from jax.experimental import pallas as pl
from jax.experimental.pallas import tpu as pltpu
from jax.sharding import PartitionSpec as P

REACH = 3
LANES = 128
norm_eps = 1e-06
LOW = -1e30


def attend_kernel(
    lo_ref, full_ref, q_ref, k3, k2, k1, k0, v3, v2, v1, v0, gate_ref, kdoc_ref, qdoc_ref,
    out_ref, k_all, v_all, m_ref, acc_ref, *, heads_pair, head_size, block_k, scale,
):
    pair, i = pl.program_id(0), pl.program_id(1)
    block_q = q_ref.shape[0]
    tok = k0.shape[0]
    pairs = k0.shape[1] // LANES

    @pl.when((pair == 0) & (i == 0))
    def _():
        for place, (k_src, v_src) in enumerate(((k3, v3), (k2, v2), (k1, v1), (k0, v0))):
            rows = pl.ds(place * tok, tok)
            k_all[rows, :] = k_src[...]
            for p in range(pairs):
                v_all[rows, pl.ds(2 * p * LANES, LANES)] = v_src[:, p * LANES : (p + 1) * LANES]
                v_all[rows, pl.ds((2 * p + 1) * LANES, LANES)] = jnp.ones(
                    (tok, LANES), v_all.dtype
                )

    own_start = REACH * tok + i * block_q
    low = lo_ref[i]
    full = full_ref[i]
    diagonal = own_start // block_k
    last = (own_start + block_q + block_k - 1) // block_k
    lane = lax.broadcasted_iota(jnp.int32, (block_q, LANES), 1)
    k_lanes = pl.ds(pl.multiple_of(pair * LANES, LANES), LANES)
    v_lanes = pl.ds(pl.multiple_of(pair * 2 * LANES, 2 * LANES), 2 * LANES)
    query = q_ref[...].astype(jnp.float32) * scale
    result = jnp.zeros((block_q, LANES), jnp.float32)
    for h in range(heads_pair):
        mine = (lane // head_size) == h
        q_head = jnp.where(mine, query, 0.0).astype(jnp.bfloat16)
        m_ref[...] = jnp.full(m_ref.shape, LOW, jnp.float32)
        acc_ref[...] = jnp.zeros(acc_ref.shape, jnp.float32)

        def step(j, masked, causal):
            start = pl.multiple_of(j * block_k, block_k)
            rows = pl.ds(start, block_k)
            score = lax.dot_general(
                q_head, k_all[rows, k_lanes], (((1,), (1,)), ((), ())),
                preferred_element_type=jnp.float32,
            )
            score = score - gate_ref[0, pl.ds(pair * heads_pair + h, 1), rows]
            if masked:
                allowed = qdoc_ref[...] == kdoc_ref[:, rows]
                if causal:
                    q_pos = own_start + lax.broadcasted_iota(jnp.int32, score.shape, 0)
                    k_pos = start + lax.broadcasted_iota(jnp.int32, score.shape, 1)
                    allowed = allowed & (k_pos <= q_pos)
                score = jnp.where(allowed, score, LOW)
            before = m_ref[...]
            top = jnp.maximum(before, jnp.max(score, axis=1, keepdims=True))
            shrink = jnp.exp(before - top)
            expo = jnp.exp(score - top[:, :1]).astype(jnp.bfloat16)
            m_ref[...] = top
            product = jnp.dot(expo, v_all[rows, v_lanes], preferred_element_type=jnp.float32)
            acc_ref[...] = acc_ref[...] * shrink[:, :1] + product

        def loop(first, end, masked, causal):
            def body(j, carry):
                step(j, masked, causal)
                return carry

            lax.fori_loop(first, end, body, 0)

        loop(low, full, True, False)
        loop(full, diagonal, False, False)
        loop(diagonal, last, True, True)
        head_out = acc_ref[:, :LANES] / acc_ref[:, LANES:]
        result = jnp.where(mine, head_out, result)
    out_ref[...] = result.astype(out_ref.dtype)


def attention(query_rows, keys, values, gates, docs, head_size):
    tok, width = query_rows.shape
    heads = gates.shape[0]
    span = (REACH + 1) * tok
    block_q = min(256, tok)
    block_k = min(512, tok)
    nq = tok // block_q
    own = docs[REACH * tok :]
    key_docs = docs.reshape(span // block_k, block_k)
    query_docs = own.reshape(nq, block_q)
    low = jnp.sum(key_docs[None, :, -1] < query_docs[:, None, 0], axis=1).astype(jnp.int32)
    full = jnp.sum(key_docs[None, :, 0] < query_docs[:, None, -1], axis=1).astype(jnp.int32)
    diagonal = (REACH * tok + jnp.arange(nq, dtype=jnp.int32) * block_q) // block_k
    full = jnp.minimum(full, diagonal)
    low = jnp.minimum(low, full)
    origin = gates[:, REACH * tok :].reshape(heads, nq, block_q)[:, :, 0]
    relative = gates[None] - origin.T[:, :, None]
    heads_pair = LANES // head_size
    vmem = pl.BlockSpec(memory_space=pltpu.VMEM)
    pairs = width // LANES
    return pl.pallas_call(
        functools.partial(
            attend_kernel,
            heads_pair=heads_pair,
            head_size=head_size,
            block_k=block_k,
            scale=head_size ** (-0.5),
        ),
        out_shape=jax.ShapeDtypeStruct((tok, width), jnp.bfloat16),
        grid_spec=pltpu.PrefetchScalarGridSpec(
            num_scalar_prefetch=2,
            grid=(pairs, nq),
            in_specs=[pl.BlockSpec((block_q, LANES), lambda p, i, *_: (i, p))]
            + [vmem] * (2 * (REACH + 1))
            + [
                pl.BlockSpec((1, heads, span), lambda p, i, *_: (i, 0, 0)),
                vmem,
                pl.BlockSpec((block_q, 1), lambda p, i, *_: (i, 0)),
            ],
            out_specs=pl.BlockSpec((block_q, LANES), lambda p, i, *_: (i, p)),
            scratch_shapes=[
                pltpu.VMEM((span, width), jnp.bfloat16),
                pltpu.VMEM((span, 2 * width), jnp.bfloat16),
                pltpu.VMEM((block_q, LANES), jnp.float32),
                pltpu.VMEM((block_q, 2 * LANES), jnp.float32),
            ],
        ),
        compiler_params=pltpu.CompilerParams(vmem_limit_bytes=40 * 1024 * 1024),
        cost_estimate=pl.CostEstimate(
            flops=16 * tok * tok * width, bytes_accessed=12 * tok * width, transcendentals=0
        ),
        name="attend",
    )(
        low, full, query_rows, *keys, *values, relative, docs[None, :], own[:, None]
    )


def send(x, axis, pairs):
    return lax.ppermute(x, axis, pairs)


def per_device(
    query_rows, key_rows, value_rows, forget_cum, doc_ids, residual, out_weight, norm_gain,
    expert_ids, route_weights, gate_proj, up_proj, down_proj,
):
    n = lax.axis_size("sp")
    parts = lax.axis_size("tp")
    s = lax.axis_index("sp")
    t = lax.axis_index("tp")
    tok, width = query_rows.shape
    heads = forget_cum.shape[0]
    head_size = width // heads
    tok_loc, model = residual.shape
    hidden_units = gate_proj.shape[2]
    piece = hidden_units // parts

    marks = jnp.concatenate([forget_cum, doc_ids.astype(jnp.float32)[None]], axis=0)
    all_marks = [marks]
    for d in range(1, REACH + 1):
        moved = send(marks, "sp", [(i, i + d) for i in range(n - d)])
        moved_docs = jnp.where(s >= d, moved[heads:], -1.0)
        all_marks.append(jnp.concatenate([moved[:heads], moved_docs], axis=0))
    all_marks = jnp.concatenate(all_marks[::-1], axis=1)

    def behind(x):
        one = send(x, "sp", [(i, i + 1) for i in range(0, n - 1, 2)])
        two = send(x, "sp", [(i, i + 2) for i in range(n - 2)])
        side = send(two, "sp", [(i, i ^ 1) for i in range(n)])
        far = send(side, "sp", [(i, i + 2) for i in range(0, n - 2, 2)])
        odd = (s % 2) == 1
        return one, two, side, far, odd

    k_one, two_k, side_k, far_k, odd = behind(key_rows)
    v_one, two_v, side_v, far_v, _ = behind(value_rows)
    keys = [jnp.where(odd, side_k, far_k), two_k, jnp.where(odd, k_one, side_k), key_rows]
    values = [jnp.where(odd, side_v, far_v), two_v, jnp.where(odd, v_one, side_v), value_rows]

    order = list(range(0, n, 2)) + list(range(1, n, 2))[::-1]
    place_of = [order.index(i) for i in range(n)]
    forward = [(order[i], order[(i + 1) % n]) for i in range(n)]
    backward = [(b, a) for a, b in forward]
    place = jnp.array(place_of, jnp.int32)[s]
    experts_in_order = jnp.array(order, jnp.int32)
    gate_up = jnp.concatenate(
        [
            lax.dynamic_slice_in_dim(gate_proj[0], t * piece, piece, 1),
            lax.dynamic_slice_in_dim(up_proj[0], t * piece, piece, 1),
        ],
        axis=1,
    )
    down = lax.dynamic_slice_in_dim(down_proj[0], t * piece, piece, 0)
    shards = [(s, gate_up, down)]
    ahead = back = (gate_up, down)
    for k in range(1, n // 2 + 1):
        ahead = tuple(send(x, "sp", forward) for x in ahead)
        shards.append((experts_in_order[(place - k) % n], *ahead))
        if k < n - n // 2:
            back = tuple(send(x, "sp", backward) for x in back)
            shards.append((experts_in_order[(place + k) % n], *back))

    high = route_weights.astype(jnp.bfloat16)
    rest = route_weights - high.astype(jnp.float32)
    middle = rest.astype(jnp.bfloat16)
    small = (rest - middle.astype(jnp.float32)).astype(jnp.bfloat16)
    routes = jnp.concatenate([expert_ids.astype(jnp.bfloat16), high, middle, small], axis=1)
    routes = jnp.pad(routes, ((0, 0), (0, LANES - routes.shape[1])))
    group_rows = lax.all_gather(
        jnp.concatenate([residual, routes], axis=1), "tp", axis=0, tiled=True
    )
    topk = expert_ids.shape[1]
    group_residual = group_rows[:, :model]
    tail = group_rows[:, model:].astype(jnp.float32)
    group_ids = tail[:, :topk]
    group_weights = (
        tail[:, topk : 2 * topk] + tail[:, 2 * topk : 3 * topk] + tail[:, 3 * topk : 4 * topk]
    )

    attended = attention(
        query_rows, keys, values, all_marks[:heads], all_marks[heads], head_size
    )

    bits = [1 << b for b in range(parts.bit_length() - 1)]
    pieces = [(0, attended)]
    for bit in bits[::-1]:
        pieces = pieces + [
            (offset ^ bit, send(x, "tp", [(i, i ^ bit) for i in range(parts)]))
            for offset, x in pieces
        ]
    heads_all = jnp.concatenate([x for _, x in pieces], axis=1)
    weight_all = jnp.concatenate(
        [
            lax.dynamic_slice_in_dim(out_weight, (t ^ offset) * width, width, 0)
            for offset, _ in pieces
        ],
        axis=0,
    )
    mixed = jnp.dot(heads_all, weight_all, preferred_element_type=jnp.float32)
    hidden = group_residual.astype(jnp.float32) + mixed
    normed = (
        hidden * lax.rsqrt(jnp.mean(hidden * hidden, axis=-1, keepdims=True) + norm_eps) * norm_gain
    ).astype(jnp.bfloat16)
    own_hidden = lax.dynamic_slice_in_dim(hidden, t * tok_loc, tok_loc, 0)

    acts = []
    for expert, both, _ in shards:
        product = jnp.dot(normed, both, preferred_element_type=jnp.float32)
        weight = jnp.sum(
            jnp.where(group_ids == expert.astype(jnp.float32), group_weights, 0.0),
            axis=1,
            keepdims=True,
        )
        act = jax.nn.silu(product[:, :piece]) * product[:, piece:]
        acts.append((act * weight).astype(jnp.bfloat16))
    acts = jnp.concatenate(acts, axis=1)
    down_all = jnp.concatenate([x for _, _, x in shards], axis=0)

    def rows_of(offset):
        return lax.dynamic_slice_in_dim(acts, (t ^ offset) * tok_loc, tok_loc, 0)

    def partial_sums(offsets):
        rows = jnp.concatenate([rows_of(o) for o in offsets], axis=0)
        return jnp.dot(rows, down_all, preferred_element_type=jnp.float32)

    keep = [0]
    for bit in bits[::-1][:-1]:
        keep = keep + [o ^ bit for o in keep]
    away = [o ^ bits[0] for o in keep]
    away_sums = partial_sums(away).astype(jnp.bfloat16)
    total = partial_sums(keep)
    total = total + send(away_sums, "tp", [(i, i ^ 1) for i in range(parts)]).astype(jnp.float32)
    rows = total.shape[0]
    for bit in bits[1:]:
        rows = rows // 2
        moved = send(
            total[rows:].astype(jnp.bfloat16), "tp", [(i, i ^ bit) for i in range(parts)]
        )
        total = total[:rows] + moved.astype(jnp.float32)
    return (own_hidden + total).astype(jnp.bfloat16)


def solution(mesh):
    placed = (
        P("sp", "tp"),
        P("sp", "tp"),
        P("sp", "tp"),
        P("tp", "sp"),
        P("sp"),
        P(("sp", "tp"), None),
        P(),
        P(),
        P(("sp", "tp"), None),
        P(("sp", "tp"), None),
        P("sp", None, None),
        P("sp", None, None),
        P("sp", None, None),
    )
    return jax.shard_map(
        per_device, mesh=mesh, in_specs=placed, out_specs=P(("sp", "tp"), None), check_vma=False
    )
```

```python
import functools

import jax
import jax.numpy as jnp
from jax import lax
from jax.experimental import pallas as pl
from jax.experimental.pallas import tpu as pltpu
from jax.sharding import PartitionSpec as P


REACH = 3
LANES = 128
norm_eps = 1e-06
LOW = -1e30


def attend_kernel(
    low_ref, full_ref, pick_ref, q_ref, *refs, sources, own, head_size, block_k, scale,
):
    pair, i = pl.program_id(0), pl.program_id(1)
    block_q = q_ref.shape[0]
    count = sum(sources)
    k_refs, v_refs = refs[:count], refs[count : 2 * count]
    gate_ref, kdoc_ref, qdoc_ref = refs[2 * count : 2 * count + 3]
    state = refs[2 * count + 3 : -4]
    k_all, v_all, m_ref, acc_ref = refs[-4:]
    tok, width = k_refs[0].shape
    pairs = width // LANES
    heads_pair = LANES // head_size

    @pl.when((pair == 0) & (i == 0))
    def _():
        def fill(place, k_src, v_src):
            rows = pl.ds(place * tok, tok)
            k_all[rows, :] = k_src[...]
            for p in range(pairs):
                v_all[rows, pl.ds(2 * p * LANES, LANES)] = v_src[:, p * LANES : (p + 1) * LANES]
                v_all[rows, pl.ds((2 * p + 1) * LANES, LANES)] = jnp.ones(
                    (tok, LANES), v_all.dtype
                )

        at = 0
        for place, options in enumerate(sources):
            if options == 1:
                fill(place, k_refs[at], v_refs[at])
            else:
                for o in range(options):
                    pl.when(pick_ref[0] == o)(
                        functools.partial(fill, place, k_refs[at + o], v_refs[at + o])
                    )
            at += options

    low, full = low_ref[i], full_ref[i]
    lane = lax.broadcasted_iota(jnp.int32, (block_q, LANES), 1)
    k_lanes = pl.ds(pl.multiple_of(pair * LANES, LANES), LANES)
    v_lanes = pl.ds(pl.multiple_of(pair * 2 * LANES, 2 * LANES), 2 * LANES)
    query = q_ref[...].astype(jnp.float32) * scale
    mine = [(lane // head_size) == h for h in range(heads_pair)]
    q_heads = [jnp.where(x, query, 0.0).astype(jnp.bfloat16) for x in mine]
    for h in range(heads_pair):
        if own:
            m_ref[h] = jnp.full((block_q, LANES), LOW, jnp.float32)
            acc_ref[h] = jnp.zeros((block_q, 2 * LANES), jnp.float32)
        else:
            m_ref[h] = jnp.broadcast_to(
                state[2][:, h * head_size : h * head_size + 1], (block_q, LANES)
            )
            acc_ref[h, :, :LANES] = state[0][...]
            acc_ref[h, :, LANES:] = state[1][...]

    def step(j, masked, causal):
        start = pl.multiple_of(j * block_k, block_k)
        rows = pl.ds(start, block_k)
        if masked:
            allowed = qdoc_ref[...] == kdoc_ref[:, rows]
            if causal:
                shape = (block_q, block_k)
                q_pos = i * block_q + lax.broadcasted_iota(jnp.int32, shape, 0)
                k_pos = start + lax.broadcasted_iota(jnp.int32, shape, 1)
                allowed = allowed & (k_pos <= q_pos)
        for h in range(heads_pair):
            score = lax.dot_general(
                q_heads[h], k_all[rows, k_lanes], (((1,), (1,)), ((), ())),
                preferred_element_type=jnp.float32,
            )
            score = score - gate_ref[0, pl.ds(pair * heads_pair + h, 1), rows]
            if masked:
                score = jnp.where(allowed, score, LOW)
            before = m_ref[h]
            top = jnp.maximum(before, jnp.max(score, axis=1, keepdims=True))
            shrink = jnp.exp(before - top)
            expo = jnp.exp(score - top[:, :1]).astype(jnp.bfloat16)
            m_ref[h] = top
            product = jnp.dot(expo, v_all[rows, v_lanes], preferred_element_type=jnp.float32)
            acc_ref[h] = acc_ref[h] * shrink[:, :1] + product

    def loop(first, end, masked, causal):
        def body(j, carry):
            step(j, masked, causal)
            return carry

        lax.fori_loop(first, end, body, 0)

    if own:
        loop(low, (i * block_q + block_q + block_k - 1) // block_k, True, True)
    else:
        loop(low, full, True, False)
        loop(full, len(sources) * tok // block_k, False, False)
    summed, total, top = (
        functools.reduce(
            lambda x, h: jnp.where(mine[h], parts[h], x), range(1, heads_pair), parts[0]
        )
        for parts in (
            [acc_ref[h, :, :LANES] for h in range(heads_pair)],
            [acc_ref[h, :, LANES:] for h in range(heads_pair)],
            [m_ref[h] for h in range(heads_pair)],
        )
    )
    if own:
        state[0][...] = summed
        state[1][...] = total
        state[2][...] = top
    else:
        state[3][...] = (summed / total).astype(state[3].dtype)


def attend(query_rows, keys, values, sources, pick, gates, key_docs, docs, head_size, state):
    own = state is None
    tok, width = query_rows.shape
    heads, span = gates.shape[1:]
    block_q = min(256, tok)
    block_k = min(512, tok)
    nq = tok // block_q
    blocked = key_docs.reshape(span // block_k, block_k)
    query_docs = docs.reshape(nq, block_q)
    low = jnp.sum(blocked[None, :, -1] < query_docs[:, None, 0], axis=1).astype(jnp.int32)
    full = jnp.sum(blocked[None, :, 0] < query_docs[:, None, -1], axis=1).astype(jnp.int32)
    if own:
        full = jnp.minimum(full, jnp.arange(nq, dtype=jnp.int32) * block_q // block_k)
    low = jnp.minimum(low, full)
    vmem = pl.BlockSpec(memory_space=pltpu.VMEM)
    pairs = width // LANES
    slab = pl.BlockSpec((block_q, LANES), lambda p, i, *_: (i, p))
    saved = jax.ShapeDtypeStruct((tok, width), jnp.float32)
    return pl.pallas_call(
        functools.partial(
            attend_kernel,
            sources=sources,
            own=own,
            head_size=head_size,
            block_k=block_k,
            scale=head_size ** (-0.5),
        ),
        out_shape=[saved] * 3 if own else jax.ShapeDtypeStruct((tok, width), jnp.bfloat16),
        grid_spec=pltpu.PrefetchScalarGridSpec(
            num_scalar_prefetch=3,
            grid=(pairs, nq),
            in_specs=[slab]
            + [vmem] * (2 * sum(sources))
            + [
                pl.BlockSpec((1, heads, span), lambda p, i, *_: (i, 0, 0)),
                vmem,
                pl.BlockSpec((block_q, 1), lambda p, i, *_: (i, 0)),
            ]
            + ([] if own else [slab] * 3),
            out_specs=[slab] * 3 if own else slab,
            scratch_shapes=[
                pltpu.VMEM((span, width), jnp.bfloat16),
                pltpu.VMEM((span, 2 * width), jnp.bfloat16),
                pltpu.VMEM((LANES // head_size, block_q, LANES), jnp.float32),
                pltpu.VMEM((LANES // head_size, block_q, 2 * LANES), jnp.float32),
            ],
        ),
        compiler_params=pltpu.CompilerParams(vmem_limit_bytes=40 * 1024 * 1024),
        cost_estimate=pl.CostEstimate(
            flops=16 * tok * span * width, bytes_accessed=12 * tok * width, transcendentals=0
        ),
        name="attend_own" if own else "attend_rest",
    )(
        low, full, pick, query_rows, *keys, *values, gates, key_docs[None, :], docs[:, None],
        *(() if own else state),
    )


def send(x, axis, pairs):
    return lax.ppermute(x, axis, pairs)


def per_device(
    query_rows, key_rows, value_rows, forget_cum, doc_ids, residual, out_weight, norm_gain,
    expert_ids, route_weights, gate_proj, up_proj, down_proj,
):
    n = lax.axis_size("sp")
    parts = lax.axis_size("tp")
    s = lax.axis_index("sp")
    t = lax.axis_index("tp")
    tok, width = query_rows.shape
    heads = forget_cum.shape[0]
    head_size = width // heads
    tok_loc, model = residual.shape
    hidden_units = gate_proj.shape[2]
    piece = hidden_units // parts

    after = lax.optimization_barrier
    flip = lambda bit: [(i, i ^ bit) for i in range(parts)]

    marks = jnp.concatenate([forget_cum, doc_ids.astype(jnp.float32)[None]], axis=0)
    moved_marks = [
        send(marks, "sp", [(i, i + d) for i in range(n - d)]) for d in range(1, REACH + 1)
    ]
    pair_kv = (key_rows, value_rows)
    two = tuple(send(x, "sp", [(i, i + 2) for i in range(n - 2)]) for x in pair_kv)
    one = tuple(send(x, "sp", [(i, i + 1) for i in range(0, n - 1, 2)]) for x in pair_kv)

    order = list(range(0, n, 2)) + list(range(1, n, 2))[::-1]
    place_of = [order.index(i) for i in range(n)]
    forward = [(order[i], order[(i + 1) % n]) for i in range(n)]
    backward = [(b, a) for a, b in forward]
    place = jnp.array(place_of, jnp.int32)[s]
    experts_in_order = jnp.array(order, jnp.int32)
    packed = jnp.concatenate(
        [
            lax.dynamic_slice_in_dim(gate_proj[0], t * piece, piece, 1),
            lax.dynamic_slice_in_dim(up_proj[0], t * piece, piece, 1),
            lax.dynamic_slice_in_dim(down_proj[0], t * piece, piece, 0).T,
        ],
        axis=1,
    )

    def ring(k, ahead, back):
        if 2 * k < n:
            return send(ahead, "sp", forward), send(back, "sp", backward)
        half = model // 2
        return jnp.concatenate(
            [send(ahead[:half], "sp", forward), send(back[half:], "sp", backward)], axis=0
        )

    shards = [(s, packed)]
    ahead, back = ring(1, packed, packed)

    high = route_weights.astype(jnp.bfloat16)
    rest = route_weights - high.astype(jnp.float32)
    middle = rest.astype(jnp.bfloat16)
    small = (rest - middle.astype(jnp.float32)).astype(jnp.bfloat16)
    routes = jnp.concatenate([expert_ids.astype(jnp.bfloat16), high, middle, small], axis=1)
    routes = jnp.pad(routes, ((0, 0), (0, LANES - routes.shape[1])))
    bits = [1 << b for b in range(parts.bit_length() - 1)]
    group = jnp.concatenate([residual, routes], axis=1)[None]
    for bit in bits[::-1]:
        group = jnp.concatenate([group, send(group, "tp", flip(bit))], axis=0)
    offsets = [0]
    for bit in bits[::-1]:
        offsets = offsets + [o ^ bit for o in offsets]
    slot_of = jnp.array([offsets.index(o) for o in range(parts)], jnp.int32)
    group_rows = jnp.concatenate(
        [lax.dynamic_index_in_dim(group, slot_of[t ^ j], 0, False) for j in range(parts)],
        axis=0,
    )
    topk = expert_ids.shape[1]
    tail = group_rows[:, model:].astype(jnp.float32)
    group_ids = tail[:, :topk]
    group_weights = (
        tail[:, topk : 2 * topk] + tail[:, 2 * topk : 3 * topk] + tail[:, 3 * topk : 4 * topk]
    )

    nq = tok // min(256, tok)
    origin = forget_cum.reshape(heads, nq, tok // nq)[:, :, 0].T[:, :, None]
    docs = doc_ids.astype(jnp.float32)
    pick = (1 - s % 2).astype(jnp.int32)[None]
    state = attend(
        query_rows, [key_rows], [value_rows], (1,), pick, forget_cum[None] - origin, docs, docs,
        head_size, None,
    )

    side = tuple(send(x, "sp", [(i, i ^ 1) for i in range(n)]) for x in two)
    far = tuple(send(x, "sp", [(i, i + 2) for i in range(0, n - 2, 2)]) for x in side)
    earlier = jnp.concatenate(moved_marks[::-1], axis=1)
    behind = jnp.repeat(jnp.arange(REACH, 0, -1, dtype=jnp.int32), tok)
    earlier_docs = jnp.where(behind <= s, earlier[heads], -1.0)
    ahead, back, far = after((ahead, back, far))
    shards += [(experts_in_order[(place - 1) % n], ahead), (experts_in_order[(place + 1) % n], back)]
    ahead, back = ring(2, ahead, back)
    attended = attend(
        query_rows,
        [side[0], far[0], two[0], one[0], side[0]],
        [side[1], far[1], two[1], one[1], side[1]],
        (2, 1, 2),
        pick,
        earlier[None, :heads] - origin,
        earlier_docs,
        docs,
        head_size,
        state,
    )

    pieces = [(0, attended)]
    for bit in bits[::-1]:
        pieces = pieces + [(o ^ bit, send(x, "tp", flip(bit))) for o, x in pieces]
    heads_all = jnp.concatenate([x for _, x in pieces], axis=1)
    weight_all = jnp.concatenate(
        [
            lax.dynamic_slice_in_dim(out_weight, (t ^ offset) * width, width, 0)
            for offset, _ in pieces
        ],
        axis=0,
    )
    mixed = jnp.dot(heads_all, weight_all, preferred_element_type=jnp.float32)
    hidden = group_rows[:, :model].astype(jnp.float32) + mixed
    normed = (
        hidden
        * lax.rsqrt(jnp.mean(hidden * hidden, axis=-1, keepdims=True) + norm_eps)
        * norm_gain
    ).astype(jnp.bfloat16)
    own_hidden = lax.dynamic_slice_in_dim(hidden, t * tok_loc, tok_loc, 0)

    def act_of(normed, expert, shard):
        product = jnp.dot(normed, shard[:, : 2 * piece], preferred_element_type=jnp.float32)
        weight = jnp.sum(
            jnp.where(group_ids == expert.astype(jnp.float32), group_weights, 0.0),
            axis=1,
            keepdims=True,
        )
        act = jax.nn.silu(product[:, :piece]) * product[:, piece:]
        return (act * weight).astype(jnp.bfloat16)

    acts = []
    for k in range(2, n // 2 + 1):
        if 2 * k < n:
            ahead, back, normed = after((ahead, back, normed))
            fresh = [
                (experts_in_order[(place - k) % n], ahead),
                (experts_in_order[(place + k) % n], back),
            ]
            following = ring(k + 1, ahead, back)
            if 2 * (k + 1) < n:
                ahead, back = following
            else:
                last = following
            acts += [act_of(normed, *x) for x in shards[len(acts) :]]
            shards += fresh
        else:
            acts += [act_of(normed, *x) for x in shards[len(acts) :]]
            last, acts[-1] = after((last, acts[-1]))
            shards.append((experts_in_order[(place + k) % n], last))
            acts.append(act_of(normed, *shards[-1]))
    acts = jnp.concatenate(acts, axis=1)
    down_all = jnp.concatenate([x[:, 2 * piece :] for _, x in shards], axis=1)

    def partial_sums(offset):
        rows = lax.dynamic_slice_in_dim(acts, (t ^ offset) * tok_loc, tok_loc, 0)
        return lax.dot_general(
            rows, down_all, (((1,), (1,)), ((), ())), preferred_element_type=jnp.float32
        )

    keep = [0]
    for bit in bits[::-1][:-1]:
        keep = keep + [o ^ bit for o in keep]
    totals = {}
    for offset in keep[::-1]:
        away = partial_sums(offset ^ bits[0]).astype(jnp.bfloat16)
        moved = send(away, "tp", flip(bits[0]))
        totals[offset] = partial_sums(offset) + moved.astype(jnp.float32)
    for bit in bits[1:]:
        for offset in [o for o in totals if o & bit]:
            moved = send(totals.pop(offset).astype(jnp.bfloat16), "tp", flip(bit))
            totals[offset ^ bit] = totals[offset ^ bit] + moved.astype(jnp.float32)
    return (own_hidden + totals[0]).astype(jnp.bfloat16)


def solution(mesh):
    placed = (
        P("sp", "tp"),
        P("sp", "tp"),
        P("sp", "tp"),
        P("tp", "sp"),
        P("sp"),
        P(("sp", "tp"), None),
        P(),
        P(),
        P(("sp", "tp"), None),
        P(("sp", "tp"), None),
        P("sp", None, None),
        P("sp", None, None),
        P("sp", None, None),
    )
    return jax.shard_map(
        per_device, mesh=mesh, in_specs=placed, out_specs=P(("sp", "tp"), None), check_vma=False
    )
```

```python
import functools

import jax
import jax.numpy as jnp
from jax import lax
from jax.experimental import pallas as pl
from jax.experimental.pallas import tpu as pltpu
from jax.sharding import PartitionSpec as P


REACH = 3
LANES = 128
norm_eps = 1e-06
LOW = -1e30


def attend_kernel(
    low_ref, full_ref, pick_ref, q_ref, *refs, sources, own, heads_pair, block_k, scale,
):
    i = pl.program_id(0)
    block_q = q_ref.shape[0]
    count = sum(sources)
    k_refs, v_refs = refs[:count], refs[count : 2 * count]
    gate_ref, kdoc_ref, qdoc_ref = refs[2 * count : 2 * count + 3]
    state = refs[2 * count + 3 : -4]
    k_all, v_all, m_ref, acc_ref = refs[-4:]
    tok = k_refs[0].shape[0]
    head_size = LANES // heads_pair

    @pl.when(i == 0)
    def _():
        v_all[:, LANES:] = jnp.ones((v_all.shape[0], LANES), v_all.dtype)

        def fill(place, k_src, v_src):
            rows = pl.ds(place * tok, tok)
            k_all[rows, :] = k_src[...]
            v_all[rows, :LANES] = v_src[...]

        at = 0
        for place, options in enumerate(sources):
            if options == 1:
                fill(place, k_refs[at], v_refs[at])
            else:
                for o in range(options):
                    pl.when(pick_ref[0] == o)(
                        functools.partial(fill, place, k_refs[at + o], v_refs[at + o])
                    )
            at += options

    low, full = low_ref[i], full_ref[i]
    lane = lax.broadcasted_iota(jnp.int32, (block_q, LANES), 1)
    query = q_ref[...].astype(jnp.float32) * scale
    mine = [(lane // head_size) == h for h in range(heads_pair)]
    q_heads = [jnp.where(x, query, 0.0).astype(jnp.bfloat16) for x in mine]
    for h in range(heads_pair):
        if own:
            m_ref[h] = jnp.full((block_q, LANES), LOW, jnp.float32)
            acc_ref[h] = jnp.zeros((block_q, 2 * LANES), jnp.float32)
        else:
            m_ref[h] = jnp.broadcast_to(
                state[2][:, h * head_size : h * head_size + 1], (block_q, LANES)
            )
            acc_ref[h, :, :LANES] = state[0][...]
            acc_ref[h, :, LANES:] = state[1][...]

    def step(j, masked, causal):
        start = pl.multiple_of(j * block_k, block_k)
        rows = pl.ds(start, block_k)
        if masked:
            allowed = qdoc_ref[...] == kdoc_ref[:, rows]
            if causal:
                shape = (block_q, block_k)
                q_pos = i * block_q + lax.broadcasted_iota(jnp.int32, shape, 0)
                k_pos = start + lax.broadcasted_iota(jnp.int32, shape, 1)
                allowed = allowed & (k_pos <= q_pos)
        for h in range(heads_pair):
            score = lax.dot_general(
                q_heads[h], k_all[rows, :], (((1,), (1,)), ((), ())),
                preferred_element_type=jnp.float32,
            )
            score = score - gate_ref[0, h : h + 1, rows]
            if masked:
                score = jnp.where(allowed, score, LOW)
            before = m_ref[h]
            top = jnp.maximum(before, jnp.max(score, axis=1, keepdims=True))
            shrink = jnp.exp(before - top)
            m_ref[h] = top
            wide = jnp.concatenate([top] * (block_k // LANES), axis=1)
            expo = jnp.exp(score - wide).astype(jnp.bfloat16)
            product = jnp.dot(expo, v_all[rows, :], preferred_element_type=jnp.float32)
            acc_ref[h] = acc_ref[h] * jnp.concatenate([shrink, shrink], axis=1) + product

    def loop(first, end, masked, causal):
        def body(j, carry):
            step(j, masked, causal)
            return carry

        lax.fori_loop(first, end, body, 0)

    if own:
        loop(low, (i * block_q + block_q + block_k - 1) // block_k, True, True)
    else:
        loop(low, full, True, False)
        loop(full, len(sources) * tok // block_k, False, False)
    summed, total, top = (
        functools.reduce(
            lambda x, h: jnp.where(mine[h], parts[h], x), range(1, heads_pair), parts[0]
        )
        for parts in (
            [acc_ref[h, :, :LANES] for h in range(heads_pair)],
            [acc_ref[h, :, LANES:] for h in range(heads_pair)],
            [m_ref[h] for h in range(heads_pair)],
        )
    )
    if own:
        state[0][...] = summed
        state[1][...] = total
        state[2][...] = top
    else:
        state[3][...] = (summed / total).astype(state[3].dtype)


BLOCK_Q = 512
BLOCK_K = 512


def visible(key_docs, docs):
    block_q, block_k = min(BLOCK_Q, docs.shape[0]), min(BLOCK_K, docs.shape[0])
    blocked = key_docs.reshape(-1, block_k)
    query_docs = docs.reshape(-1, block_q)
    low = jnp.sum(blocked[None, :, -1] < query_docs[:, None, 0], axis=1).astype(jnp.int32)
    full = jnp.sum(blocked[None, :, 0] < query_docs[:, None, -1], axis=1).astype(jnp.int32)
    return low, full


def attend(pair, query_rows, blocks, sources, pick, bounds, gates, key_docs, docs, head_size, state):
    own = state is None
    tok = query_rows.shape[0]
    span = gates.shape[2]
    block_q, block_k = min(BLOCK_Q, tok), min(BLOCK_K, tok)
    nq = tok // block_q
    heads_pair = LANES // head_size
    slab = pl.BlockSpec((block_q, LANES), lambda i, *_: (i, 0))
    saved = jax.ShapeDtypeStruct((tok, LANES), jnp.float32)

    def column(at):
        return pl.BlockSpec((tok, LANES), lambda i, *_: (0, at))

    return pl.pallas_call(
        functools.partial(
            attend_kernel,
            sources=sources,
            own=own,
            heads_pair=heads_pair,
            block_k=block_k,
            scale=head_size ** (-0.5),
        ),
        out_shape=[saved] * 3 if own else jax.ShapeDtypeStruct((tok, LANES), jnp.bfloat16),
        grid_spec=pltpu.PrefetchScalarGridSpec(
            num_scalar_prefetch=3,
            grid=(nq,),
            in_specs=[pl.BlockSpec((block_q, LANES), lambda i, *_: (i, pair))]
            + [column(x[1]) for x in blocks]
            + [column(x[3]) for x in blocks]
            + [
                pl.BlockSpec((1, heads_pair, span), lambda i, *_: (i, 0, 0)),
                pl.BlockSpec((1, span), lambda i, *_: (0, 0)),
                pl.BlockSpec((block_q, 1), lambda i, *_: (i, 0)),
            ]
            + ([] if own else [slab] * 3),
            out_specs=[slab] * 3 if own else slab,
            scratch_shapes=[
                pltpu.VMEM((span, LANES), jnp.bfloat16),
                pltpu.VMEM((span, 2 * LANES), jnp.bfloat16),
                pltpu.VMEM((heads_pair, block_q, LANES), jnp.float32),
                pltpu.VMEM((heads_pair, block_q, 2 * LANES), jnp.float32),
            ],
        ),
        compiler_params=pltpu.CompilerParams(vmem_limit_bytes=32 * 1024 * 1024),
        cost_estimate=pl.CostEstimate(
            flops=16 * tok * span * LANES, bytes_accessed=12 * tok * LANES, transcendentals=0
        ),
        name="attend_own" if own else "attend_rest",
    )(
        *bounds, pick, query_rows, *[x[0] for x in blocks], *[x[2] for x in blocks],
        gates[:, pair * heads_pair : (pair + 1) * heads_pair], key_docs[None, :], docs[:, None],
        *(() if own else state),
    )


def send(x, axis, pairs):
    return lax.ppermute(x, axis, pairs)


def per_device(
    query_rows, key_rows, value_rows, forget_cum, doc_ids, residual, out_weight, norm_gain,
    expert_ids, route_weights, gate_proj, up_proj, down_proj,
):
    n = lax.axis_size("sp")
    parts = lax.axis_size("tp")
    s = lax.axis_index("sp")
    t = lax.axis_index("tp")
    tok, width = query_rows.shape
    heads = forget_cum.shape[0]
    head_size = width // heads
    tok_loc, model = residual.shape
    hidden_units = gate_proj.shape[2]
    piece = hidden_units // parts

    flip = lambda bit: [(i, i ^ bit) for i in range(parts)]

    rows_kv = jnp.concatenate([key_rows, value_rows], axis=1)
    one = send(rows_kv, "sp", [(i, i + 1) for i in range(n - 1)])
    two = send(rows_kv, "sp", [(i, i + 2) for i in range(n - 2)])
    marks = jnp.concatenate([forget_cum, doc_ids.astype(jnp.float32)[None]], axis=0)
    moved_marks = [
        send(marks, "sp", [(i, i + d) for i in range(n - d)]) for d in range(1, REACH + 1)
    ]
    far = send(one, "sp", [(i, i + 2) for i in range(0, n - 2, 2)])
    side = send(two, "sp", [(i, i + 1) for i in range(0, n - 1, 2)])

    def expert_at(place):
        place = (place + n) % n
        return jnp.where(place < (n + 1) // 2, 2 * place, 2 * (n - 1 - place) + 1)

    order = list(range(0, n, 2)) + list(range(1, n, 2))[::-1]
    forward = [(order[i], order[(i + 1) % n]) for i in range(n)]
    backward = [(b, a) for a, b in forward]
    place = jnp.where(s % 2 == 0, s // 2, n - 1 - s // 2)
    gate_up = jnp.concatenate(
        [
            lax.dynamic_slice_in_dim(gate_proj[0], t * piece, piece, 1),
            lax.dynamic_slice_in_dim(up_proj[0], t * piece, piece, 1),
        ],
        axis=1,
    )
    down = lax.dynamic_slice_in_dim(down_proj[0], t * piece, piece, 0)

    def ring(k, ahead, back):
        if 2 * k < n:
            return send(ahead, "sp", forward), send(back, "sp", backward)
        half = ahead.shape[0] // 2
        return send(ahead[:half], "sp", forward), send(back[half:], "sp", backward)

    steps = n // 2
    wide = {1: ring(1, gate_up, gate_up)}
    flat = {1: ring(1, down, down)}

    high = route_weights.astype(jnp.bfloat16)
    rest = route_weights - high.astype(jnp.float32)
    middle = rest.astype(jnp.bfloat16)
    small = (rest - middle.astype(jnp.float32)).astype(jnp.bfloat16)
    routes = jnp.concatenate([expert_ids.astype(jnp.bfloat16), high, middle, small], axis=1)
    routes = jnp.pad(routes, ((0, 0), (0, LANES - routes.shape[1])))
    bits = [1 << b for b in range(parts.bit_length() - 1)]
    group = [(0, jnp.concatenate([residual, routes], axis=1))]
    for bit in bits[::-1]:
        group = group + [(o ^ bit, send(x, "tp", flip(bit))) for o, x in group]
    group_rows = jnp.zeros((tok, model + LANES), jnp.bfloat16)
    for o, x in group:
        group_rows = lax.dynamic_update_slice_in_dim(group_rows, x, (t ^ o) * tok_loc, 0)
    topk = expert_ids.shape[1]
    tail = group_rows[:, model:].astype(jnp.float32)
    group_ids = tail[:, :topk]
    group_weights = (
        tail[:, topk : 2 * topk] + tail[:, 2 * topk : 3 * topk] + tail[:, 3 * topk : 4 * topk]
    )

    nq = tok // min(BLOCK_Q, tok)
    pairs = width // LANES
    origin = forget_cum.reshape(heads, nq, tok // nq)[:, :, 0].T[:, :, None]
    docs = doc_ids.astype(jnp.float32)
    pick = (1 - s % 2).astype(jnp.int32)[None]
    own_bounds = visible(docs, docs)
    states = [
        attend(
            p, query_rows, [(key_rows, p, value_rows, p)], (1,), pick, own_bounds,
            forget_cum[None] - origin, docs, docs, head_size, None,
        )
        for p in range(pairs)
    ]
    earlier = jnp.concatenate(moved_marks[::-1], axis=1)
    behind = lax.broadcasted_iota(jnp.int32, (REACH, tok), 0).reshape(-1)
    earlier_docs = jnp.where(REACH - behind <= s, earlier[heads], -1.0)
    bounds = visible(earlier_docs, docs)
    relative = earlier[None, :heads] - origin
    attended = []
    for p in range(pairs):
        attended.append(
            attend(
                p, query_rows, [(x, p, x, pairs + p) for x in (side, far, two, one)],
                (2, 1, 1), pick, bounds, relative, earlier_docs, docs, head_size, states[p],
            )
        )
    wide[2] = ring(2, *wide[1])
    flat[2] = ring(2, *flat[1])

    pieces = [(0, tuple(attended))]
    for bit in bits[::-1]:
        pieces = pieces + [(o ^ bit, tuple(send(y, "tp", flip(bit)) for y in x)) for o, x in pieces]
    heads_all = jnp.concatenate([y for _, x in pieces for y in x], axis=1)
    weight_all = jnp.concatenate(
        [
            lax.dynamic_slice_in_dim(out_weight, (t ^ offset) * width, width, 0)
            for offset, _ in pieces
        ],
        axis=0,
    )
    mixed = jnp.dot(heads_all, weight_all, preferred_element_type=jnp.float32)
    hidden = group_rows[:, :model].astype(jnp.float32) + mixed
    normed = (
        hidden
        * lax.rsqrt(jnp.mean(hidden * hidden, axis=-1, keepdims=True) + norm_eps)
        * norm_gain
    ).astype(jnp.bfloat16)
    own_hidden = lax.dynamic_slice_in_dim(hidden, t * tok_loc, tok_loc, 0)

    def act_of(normed, expert, shard):
        product = jnp.dot(normed, shard, preferred_element_type=jnp.float32)
        weight = jnp.sum(
            jnp.where(group_ids == expert.astype(jnp.float32), group_weights, 0.0),
            axis=1,
            keepdims=True,
        )
        act = jax.nn.silu(product[:, :piece]) * product[:, piece:]
        return (act * weight).astype(jnp.bfloat16)

    for k in range(3, steps + 1):
        wide[k] = ring(k, *wide[k - 1])
        flat[k] = ring(k, *flat[k - 1])
    acts, downs = [], []
    for k in range(steps + 1):
        if k == 0:
            shards = [(place, gate_up, down)]
        elif 2 * k < n:
            shards = [
                (place - k, wide[k][0], flat[k][0]),
                (place + k, wide[k][1], flat[k][1]),
            ]
        else:
            shards = [
                (place + k, jnp.concatenate(wide[k], axis=0), jnp.concatenate(flat[k], axis=0))
            ]
        for where, shard, lower in shards:
            acts.append(act_of(normed, expert_at(where), shard))
            downs.append(lower)
    acts = jnp.concatenate(acts, axis=1)
    down_all = jnp.concatenate(downs, axis=0)

    def partial_sums(offset):
        rows = lax.dynamic_slice_in_dim(acts, (t ^ offset) * tok_loc, tok_loc, 0)
        return jnp.dot(rows, down_all, preferred_element_type=jnp.float32)

    keep = [0]
    for bit in bits[::-1][:-1]:
        keep = keep + [o ^ bit for o in keep]
    totals = {}
    for offset in keep[::-1]:
        away = partial_sums(offset ^ bits[0]).astype(jnp.bfloat16)
        moved = send(away, "tp", flip(bits[0]))
        totals[offset] = partial_sums(offset) + moved.astype(jnp.float32)
    for bit in bits[1:]:
        for offset in [o for o in totals if o & bit]:
            moved = send(totals.pop(offset).astype(jnp.bfloat16), "tp", flip(bit))
            totals[offset ^ bit] = totals[offset ^ bit] + moved.astype(jnp.float32)
    return (own_hidden + totals[0]).astype(jnp.bfloat16)


def solution(mesh):
    placed = (
        P("sp", "tp"),
        P("sp", "tp"),
        P("sp", "tp"),
        P("tp", "sp"),
        P("sp"),
        P(("sp", "tp"), None),
        P(),
        P(),
        P(("sp", "tp"), None),
        P(("sp", "tp"), None),
        P("sp", None, None),
        P("sp", None, None),
        P("sp", None, None),
    )
    return jax.shard_map(
        per_device, mesh=mesh, in_specs=placed, out_specs=P(("sp", "tp"), None), check_vma=False
    )
```

```python
import functools

import jax
import jax.numpy as jnp
from jax import lax
from jax.experimental import pallas as pl
from jax.experimental.pallas import tpu as pltpu
from jax.sharding import PartitionSpec as P


REACH = 3
LANES = 128
norm_eps = 1e-06
LOW = -1e30


def attend_kernel(
    low_ref, full_ref, pick_ref, q_ref, *refs, sources, own, heads_pair, block_k, scale,
):
    i = pl.program_id(0)
    block_q = q_ref.shape[0]
    count = sum(sources)
    k_refs, v_refs = refs[:count], refs[count : 2 * count]
    gate_ref, kdoc_ref, qdoc_ref = refs[2 * count : 2 * count + 3]
    state = refs[2 * count + 3 : -4]
    k_all, v_all, m_ref, acc_ref = refs[-4:]
    tok = k_refs[0].shape[0]
    head_size = LANES // heads_pair

    @pl.when(i == 0)
    def _():
        v_all[:, LANES:] = jnp.ones((v_all.shape[0], LANES), v_all.dtype)

        def fill(place, k_src, v_src):
            rows = pl.ds(place * tok, tok)
            k_all[rows, :] = k_src[...]
            v_all[rows, :LANES] = v_src[...]

        at = 0
        for place, options in enumerate(sources):
            if options == 1:
                fill(place, k_refs[at], v_refs[at])
            else:
                for o in range(options):
                    pl.when(pick_ref[0] == o)(
                        functools.partial(fill, place, k_refs[at + o], v_refs[at + o])
                    )
            at += options

    low, full = low_ref[i], full_ref[i]
    lane = lax.broadcasted_iota(jnp.int32, (block_q, LANES), 1)
    query = q_ref[...].astype(jnp.float32) * scale
    mine = [(lane // head_size) == h for h in range(heads_pair)]
    q_heads = [jnp.where(x, query, 0.0).astype(jnp.bfloat16) for x in mine]
    for h in range(heads_pair):
        if own:
            m_ref[h] = jnp.full((block_q, LANES), LOW, jnp.float32)
            acc_ref[h] = jnp.zeros((block_q, 2 * LANES), jnp.float32)
        else:
            m_ref[h] = jnp.broadcast_to(
                state[2][:, h * head_size : h * head_size + 1], (block_q, LANES)
            )
            acc_ref[h, :, :LANES] = state[0][...]
            acc_ref[h, :, LANES:] = state[1][...]

    def step(j, masked, causal):
        start = pl.multiple_of(j * block_k, block_k)
        rows = pl.ds(start, block_k)
        if masked:
            allowed = qdoc_ref[...] == kdoc_ref[:, rows]
            if causal:
                shape = (block_q, block_k)
                q_pos = i * block_q + lax.broadcasted_iota(jnp.int32, shape, 0)
                k_pos = start + lax.broadcasted_iota(jnp.int32, shape, 1)
                allowed = allowed & (k_pos <= q_pos)
        for h in range(heads_pair):
            score = lax.dot_general(
                q_heads[h], k_all[rows, :], (((1,), (1,)), ((), ())),
                preferred_element_type=jnp.float32,
            )
            score = score - gate_ref[0, h : h + 1, rows]
            if masked:
                score = jnp.where(allowed, score, LOW)
            before = m_ref[h]
            top = jnp.maximum(before, jnp.max(score, axis=1, keepdims=True))
            shrink = jnp.exp(before - top)
            m_ref[h] = top
            wide = jnp.concatenate([top] * (block_k // LANES), axis=1)
            expo = jnp.exp(score - wide).astype(jnp.bfloat16)
            product = jnp.dot(expo, v_all[rows, :], preferred_element_type=jnp.float32)
            acc_ref[h] = acc_ref[h] * jnp.concatenate([shrink, shrink], axis=1) + product

    def loop(first, end, masked, causal):
        def body(j, carry):
            step(j, masked, causal)
            return carry

        lax.fori_loop(first, end, body, 0)

    if own:
        loop(low, (i * block_q + block_q + block_k - 1) // block_k, True, True)
    else:
        loop(low, full, True, False)
        loop(full, len(sources) * tok // block_k, False, False)
    summed, total, top = (
        functools.reduce(
            lambda x, h: jnp.where(mine[h], parts[h], x), range(1, heads_pair), parts[0]
        )
        for parts in (
            [acc_ref[h, :, :LANES] for h in range(heads_pair)],
            [acc_ref[h, :, LANES:] for h in range(heads_pair)],
            [m_ref[h] for h in range(heads_pair)],
        )
    )
    if own:
        state[0][...] = summed
        state[1][...] = total
        state[2][...] = top
    else:
        state[3][...] = (summed / total).astype(state[3].dtype)


BLOCK_Q = 512
BLOCK_K = 512


def visible(key_docs, docs):
    block_q, block_k = min(BLOCK_Q, docs.shape[0]), min(BLOCK_K, docs.shape[0])
    blocked = key_docs.reshape(-1, block_k)
    query_docs = docs.reshape(-1, block_q)
    low = jnp.sum(blocked[None, :, -1] < query_docs[:, None, 0], axis=1).astype(jnp.int32)
    full = jnp.sum(blocked[None, :, 0] < query_docs[:, None, -1], axis=1).astype(jnp.int32)
    return low, full


def attend(pair, query_rows, blocks, sources, pick, bounds, gates, key_docs, docs, head_size, state):
    own = state is None
    tok = query_rows.shape[0]
    span = gates.shape[2]
    block_q, block_k = min(BLOCK_Q, tok), min(BLOCK_K, tok)
    nq = tok // block_q
    heads_pair = LANES // head_size
    slab = pl.BlockSpec((block_q, LANES), lambda i, *_: (i, 0))
    saved = jax.ShapeDtypeStruct((tok, LANES), jnp.float32)

    def column(at):
        return pl.BlockSpec((tok, LANES), lambda i, *_: (at, pair))

    return pl.pallas_call(
        functools.partial(
            attend_kernel,
            sources=sources,
            own=own,
            heads_pair=heads_pair,
            block_k=block_k,
            scale=head_size ** (-0.5),
        ),
        out_shape=[saved] * 3 if own else jax.ShapeDtypeStruct((tok, LANES), jnp.bfloat16),
        grid_spec=pltpu.PrefetchScalarGridSpec(
            num_scalar_prefetch=3,
            grid=(nq,),
            in_specs=[pl.BlockSpec((block_q, LANES), lambda i, *_: (i, pair))]
            + [column(x[1]) for x in blocks]
            + [column(x[3]) for x in blocks]
            + [
                pl.BlockSpec((1, heads_pair, span), lambda i, *_: (i, 0, 0)),
                pl.BlockSpec((1, span), lambda i, *_: (0, 0)),
                pl.BlockSpec((block_q, 1), lambda i, *_: (i, 0)),
            ]
            + ([] if own else [slab] * 3),
            out_specs=[slab] * 3 if own else slab,
            scratch_shapes=[
                pltpu.VMEM((span, LANES), jnp.bfloat16),
                pltpu.VMEM((span, 2 * LANES), jnp.bfloat16),
                pltpu.VMEM((heads_pair, block_q, LANES), jnp.float32),
                pltpu.VMEM((heads_pair, block_q, 2 * LANES), jnp.float32),
            ],
        ),
        compiler_params=pltpu.CompilerParams(vmem_limit_bytes=32 * 1024 * 1024),
        cost_estimate=pl.CostEstimate(
            flops=16 * tok * span * LANES, bytes_accessed=12 * tok * LANES, transcendentals=0
        ),
        name="attend_own" if own else "attend_rest",
    )(
        *bounds, pick, query_rows, *[x[0] for x in blocks], *[x[2] for x in blocks],
        gates[:, pair * heads_pair : (pair + 1) * heads_pair], key_docs[None, :], docs[:, None],
        *(() if own else state),
    )


def send(x, axis, pairs):
    return lax.ppermute(x, axis, pairs)


def three_parts(x):
    high = lax.reduce_precision(x, 8, 7)
    middle = lax.reduce_precision(x - high, 8, 7)
    low = x - high - middle
    return [y.astype(jnp.bfloat16) for y in (high, middle, low)]


def per_device(
    query_rows, key_rows, value_rows, forget_cum, doc_ids, residual, out_weight, norm_gain,
    expert_ids, route_weights, gate_proj, up_proj, down_proj,
):
    n = lax.axis_size("sp")
    parts = lax.axis_size("tp")
    s = lax.axis_index("sp")
    t = lax.axis_index("tp")
    tok, width = query_rows.shape
    heads = forget_cum.shape[0]
    head_size = width // heads
    tok_loc, model = residual.shape
    hidden_units = gate_proj.shape[2]
    piece = hidden_units // parts

    after = lax.optimization_barrier
    flip = lambda bit: [(i, i ^ bit) for i in range(parts)]

    marks = jnp.concatenate([*three_parts(forget_cum), doc_ids[None].astype(jnp.bfloat16)])
    marks = jnp.pad(marks, ((0, 4 * heads - marks.shape[0]), (0, 0))).reshape(-1, width)
    rows_kv = jnp.concatenate([key_rows, value_rows, marks], axis=0)
    one = send(rows_kv, "sp", [(i, i + 1) for i in range(n - 1)])
    two = send(rows_kv, "sp", [(i, i + 2) for i in range(n - 2)])
    far = send(one, "sp", [(i, i + 2) for i in range(0, n - 2, 2)])
    side = send(two, "sp", [(i, i + 1) for i in range(0, n - 1, 2)])
    odd = s % 2 == 1

    def expert_at(place):
        place = (place + n) % n
        return jnp.where(place < (n + 1) // 2, 2 * place, 2 * (n - 1 - place) + 1)

    order = list(range(0, n, 2)) + list(range(1, n, 2))[::-1]
    forward = [(order[i], order[(i + 1) % n]) for i in range(n)]
    backward = [(b, a) for a, b in forward]
    place = jnp.where(s % 2 == 0, s // 2, n - 1 - s // 2)
    gate_up = jnp.concatenate(
        [
            lax.dynamic_slice_in_dim(gate_proj[0], t * piece, piece, 1),
            lax.dynamic_slice_in_dim(up_proj[0], t * piece, piece, 1),
        ],
        axis=1,
    )
    down = lax.dynamic_slice_in_dim(down_proj[0], t * piece, piece, 0)

    def ring(k, ahead, back):
        if 2 * k < n:
            return send(ahead, "sp", forward), send(back, "sp", backward)
        half = ahead.shape[0] // 2
        return send(ahead[:half], "sp", forward), send(back[half:], "sp", backward)

    steps = n // 2
    wide = {1: ring(1, gate_up, gate_up)}
    flat = {1: ring(1, down, down)}

    routes = jnp.concatenate([expert_ids.astype(jnp.bfloat16), *three_parts(route_weights)], axis=1)
    routes = jnp.pad(routes, ((0, 0), (0, LANES - routes.shape[1])))
    bits = [1 << b for b in range(parts.bit_length() - 1)]
    group = [(0, jnp.concatenate([residual, routes], axis=1))]
    for bit in bits[::-1]:
        group = group + [(o ^ bit, send(x, "tp", flip(bit))) for o, x in group]
    group_rows = jnp.zeros((tok, model + LANES), jnp.bfloat16)
    for o, x in group:
        group_rows = lax.dynamic_update_slice_in_dim(group_rows, x, (t ^ o) * tok_loc, 0)
    topk = expert_ids.shape[1]
    tail = group_rows[:, model:].astype(jnp.float32)
    group_ids = tail[:, :topk]
    group_weights = (
        tail[:, topk : 2 * topk] + tail[:, 2 * topk : 3 * topk] + tail[:, 3 * topk : 4 * topk]
    )

    nq = tok // min(BLOCK_Q, tok)
    pairs = width // LANES
    origin = forget_cum.reshape(heads, nq, tok // nq)[:, :, 0].T[:, :, None]
    docs = doc_ids.astype(jnp.float32)
    pick = jnp.where(odd, 0, 1).astype(jnp.int32)[None]
    own_bounds = visible(docs, docs)
    states = [
        attend(
            p, query_rows, [(key_rows, 0, value_rows, 0)], (1,), pick, own_bounds,
            forget_cum[None] - origin, docs, docs, head_size, None,
        )
        for p in range(pairs)
    ]
    third = jnp.where(odd, side[2 * tok :], far[2 * tok :])
    sent = [x.reshape(-1, tok).astype(jnp.float32) for x in (third, two[2 * tok :], one[2 * tok :])]
    earlier = jnp.concatenate(
        [x[:heads] + x[heads : 2 * heads] + x[2 * heads : 3 * heads] for x in sent], axis=1
    )
    earlier_docs = jnp.concatenate(
        [jnp.where(REACH - i <= s, x[3 * heads], -1.0) for i, x in enumerate(sent)]
    )
    bounds = visible(earlier_docs, docs)
    relative = earlier[None] - origin
    attended = []
    for p in range(pairs):
        attended.append(
            attend(
                p, query_rows, [(x, 0, x, 1) for x in (side, far, two, one)], (2, 1, 1),
                pick, bounds, relative, earlier_docs, docs, head_size, states[p],
            )
        )
    wide[2] = ring(2, *wide[1])
    flat[2] = ring(2, *flat[1])

    pieces = [(0, tuple(attended))]
    for bit in bits[::-1]:
        pieces = pieces + [(o ^ bit, tuple(send(y, "tp", flip(bit)) for y in x)) for o, x in pieces]
    heads_all = jnp.concatenate([y for _, x in pieces for y in x], axis=1)
    weight_all = jnp.concatenate(
        [
            lax.dynamic_slice_in_dim(out_weight, (t ^ offset) * width, width, 0)
            for offset, _ in pieces
        ],
        axis=0,
    )
    mixed = jnp.dot(heads_all, weight_all, preferred_element_type=jnp.float32)
    hidden = group_rows[:, :model].astype(jnp.float32) + mixed
    normed = (
        hidden
        * lax.rsqrt(jnp.mean(hidden * hidden, axis=-1, keepdims=True) + norm_eps)
        * norm_gain
    ).astype(jnp.bfloat16)
    own_hidden = lax.dynamic_slice_in_dim(hidden, t * tok_loc, tok_loc, 0)

    def act_of(normed, expert, shard):
        product = jnp.dot(normed, shard, preferred_element_type=jnp.float32)
        weight = jnp.sum(
            jnp.where(group_ids == expert.astype(jnp.float32), group_weights, 0.0),
            axis=1,
            keepdims=True,
        )
        act = jax.nn.silu(product[:, :piece]) * product[:, piece:]
        return (act * weight).astype(jnp.bfloat16)

    for k in range(3, steps + 1):
        wide[k] = ring(k, *wide[k - 1])
        flat[k] = ring(k, *flat[k - 1])
    acts, downs = [], []
    for k in range(steps + 1):
        if k == 0:
            shards = [(place, gate_up, down)]
        elif 2 * k < n:
            shards = [
                (place - k, wide[k][0], flat[k][0]),
                (place + k, wide[k][1], flat[k][1]),
            ]
        else:
            shards = [
                (place + k, jnp.concatenate(wide[k], axis=0), jnp.concatenate(flat[k], axis=0))
            ]
        for where, shard, lower in shards:
            acts.append(act_of(normed, expert_at(where), shard))
            downs.append(lower)
    early = jnp.dot(
        jnp.concatenate(acts[:-1], axis=1),
        jnp.concatenate(downs[:-1], axis=0),
        preferred_element_type=jnp.float32,
    )

    def partial_sums(offset):
        first = (t ^ offset) * tok_loc
        rows = lax.dynamic_slice_in_dim(acts[-1], first, tok_loc, 0)
        product = jnp.dot(rows, downs[-1], preferred_element_type=jnp.float32)
        return product + lax.dynamic_slice_in_dim(early, first, tok_loc, 0)

    keep = [0]
    for bit in bits[::-1][:-1]:
        keep = keep + [o ^ bit for o in keep]
    totals = {}
    for offset in keep[::-1]:
        away = partial_sums(offset ^ bits[0]).astype(jnp.bfloat16)
        moved = send(away, "tp", flip(bits[0]))
        totals[offset] = partial_sums(offset) + moved.astype(jnp.float32)
    totals[0] = totals[0] + own_hidden
    for bit in bits[1:]:
        for offset in [o for o in totals if o & bit]:
            moved = send(totals.pop(offset).astype(jnp.bfloat16), "tp", flip(bit))
            ready, moved = after((totals[offset ^ bit], moved))
            totals[offset ^ bit] = ready + moved.astype(jnp.float32)
    return totals[0].astype(jnp.bfloat16)


def solution(mesh):
    placed = (
        P("sp", "tp"),
        P("sp", "tp"),
        P("sp", "tp"),
        P("tp", "sp"),
        P("sp"),
        P(("sp", "tp"), None),
        P(),
        P(),
        P(("sp", "tp"), None),
        P(("sp", "tp"), None),
        P("sp", None, None),
        P("sp", None, None),
        P("sp", None, None),
    )
    return jax.shard_map(
        per_device, mesh=mesh, in_specs=placed, out_specs=P(("sp", "tp"), None), check_vma=False
    )
```

```python
import functools

import jax
import jax.numpy as jnp
from jax import lax
from jax.experimental import pallas as pl
from jax.experimental.pallas import tpu as pltpu
from jax.sharding import PartitionSpec as P


REACH = 3
LANES = 128
norm_eps = 1e-06
LOW = -1e30
VMEM_LIMIT = 32 * 1024 * 1024


def attend_kernel(
    low_ref, full_ref, pick_ref, q_ref, *refs, sources, own, heads_pair, block_k, scale,
):
    i = pl.program_id(0)
    block_q = q_ref.shape[0]
    count = sum(sources)
    k_refs, v_refs = refs[:count], refs[count : 2 * count]
    gate_ref, kdoc_ref, qdoc_ref = refs[2 * count : 2 * count + 3]
    state = refs[2 * count + 3 : -4]
    k_all, v_all, m_ref, acc_ref = refs[-4:]
    tok = k_refs[0].shape[0]
    head_size = LANES // heads_pair

    @pl.when(i == 0)
    def _():
        v_all[:, LANES:] = jnp.ones((v_all.shape[0], LANES), v_all.dtype)

        def fill(place, k_src, v_src):
            rows = pl.ds(place * tok, tok)
            k_all[rows, :] = k_src[...]
            v_all[rows, :LANES] = v_src[...]

        at = 0
        for place, options in enumerate(sources):
            if options == 1:
                fill(place, k_refs[at], v_refs[at])
            else:
                for o in range(options):
                    pl.when(pick_ref[0] == o)(
                        functools.partial(fill, place, k_refs[at + o], v_refs[at + o])
                    )
            at += options

    low, full = low_ref[i], full_ref[i]
    lane = lax.broadcasted_iota(jnp.int32, (block_q, LANES), 1)
    query = q_ref[...].astype(jnp.float32) * scale
    mine = [(lane // head_size) == h for h in range(heads_pair)]
    q_heads = [jnp.where(x, query, 0.0).astype(jnp.bfloat16) for x in mine]
    for h in range(heads_pair):
        if own:
            m_ref[h] = jnp.full((block_q, LANES), LOW, jnp.float32)
            acc_ref[h] = jnp.zeros((block_q, 2 * LANES), jnp.float32)
        else:
            m_ref[h] = jnp.broadcast_to(
                state[2][:, h * head_size : h * head_size + 1], (block_q, LANES)
            )
            acc_ref[h, :, :LANES] = state[0][...]
            acc_ref[h, :, LANES:] = state[1][...]

    def step(j, masked, causal):
        start = pl.multiple_of(j * block_k, block_k)
        rows = pl.ds(start, block_k)
        if masked:
            allowed = qdoc_ref[...] == kdoc_ref[:, rows]
            if causal:
                shape = (block_q, block_k)
                q_pos = i * block_q + lax.broadcasted_iota(jnp.int32, shape, 0)
                k_pos = start + lax.broadcasted_iota(jnp.int32, shape, 1)
                allowed = allowed & (k_pos <= q_pos)
        for h in range(heads_pair):
            score = lax.dot_general(
                q_heads[h], k_all[rows, :], (((1,), (1,)), ((), ())),
                preferred_element_type=jnp.float32,
            )
            score = score - gate_ref[0, h : h + 1, rows]
            if masked:
                score = jnp.where(allowed, score, LOW)
            before = m_ref[h]
            top = jnp.maximum(before, jnp.max(score, axis=1, keepdims=True))
            shrink = jnp.exp(before - top)
            m_ref[h] = top
            wide = jnp.concatenate([top] * (block_k // LANES), axis=1)
            expo = jnp.exp(score - wide).astype(jnp.bfloat16)
            product = jnp.dot(expo, v_all[rows, :], preferred_element_type=jnp.float32)
            acc_ref[h] = acc_ref[h] * jnp.concatenate([shrink, shrink], axis=1) + product

    def loop(first, end, masked, causal):
        def body(j, carry):
            step(j, masked, causal)
            return carry

        lax.fori_loop(first, end, body, 0)

    if own:
        loop(low, (i * block_q + block_q + block_k - 1) // block_k, True, True)
    else:
        loop(low, full, True, False)
        loop(full, len(sources) * tok // block_k, False, False)
    summed, total, top = (
        functools.reduce(
            lambda x, h: jnp.where(mine[h], parts[h], x), range(1, heads_pair), parts[0]
        )
        for parts in (
            [acc_ref[h, :, :LANES] for h in range(heads_pair)],
            [acc_ref[h, :, LANES:] for h in range(heads_pair)],
            [m_ref[h] for h in range(heads_pair)],
        )
    )
    if own:
        state[0][...] = summed
        state[1][...] = total
        state[2][...] = top
    else:
        state[3][...] = (summed / total).astype(state[3].dtype)


BLOCK_Q = 512
BLOCK_K = 512


def visible(key_docs, docs):
    block_q, block_k = min(BLOCK_Q, docs.shape[0]), min(BLOCK_K, docs.shape[0])
    blocked = key_docs.reshape(-1, block_k)
    query_docs = docs.reshape(-1, block_q)
    low = jnp.sum(blocked[None, :, -1] < query_docs[:, None, 0], axis=1).astype(jnp.int32)
    full = jnp.sum(blocked[None, :, 0] < query_docs[:, None, -1], axis=1).astype(jnp.int32)
    return low, full


def attend(pair, query_rows, blocks, sources, pick, bounds, gates, key_docs, docs, head_size, state):
    own = state is None
    tok = query_rows.shape[0]
    span = gates.shape[2]
    block_q, block_k = min(BLOCK_Q, tok), min(BLOCK_K, tok)
    nq = tok // block_q
    heads_pair = LANES // head_size
    slab = pl.BlockSpec((block_q, LANES), lambda i, *_: (i, 0))
    saved = jax.ShapeDtypeStruct((tok, LANES), jnp.float32)

    def column(at):
        return pl.BlockSpec((tok, LANES), lambda i, *_: (at, pair))

    return pl.pallas_call(
        functools.partial(
            attend_kernel,
            sources=sources,
            own=own,
            heads_pair=heads_pair,
            block_k=block_k,
            scale=head_size ** (-0.5),
        ),
        out_shape=[saved] * 3 if own else jax.ShapeDtypeStruct((tok, LANES), jnp.bfloat16),
        grid_spec=pltpu.PrefetchScalarGridSpec(
            num_scalar_prefetch=3,
            grid=(nq,),
            in_specs=[pl.BlockSpec((block_q, LANES), lambda i, *_: (i, pair))]
            + [column(x[1]) for x in blocks]
            + [column(x[3]) for x in blocks]
            + [
                pl.BlockSpec((1, heads_pair, span), lambda i, *_: (i, 0, 0)),
                pl.BlockSpec((1, span), lambda i, *_: (0, 0)),
                pl.BlockSpec((block_q, 1), lambda i, *_: (i, 0)),
            ]
            + ([] if own else [slab] * 3),
            out_specs=[slab] * 3 if own else slab,
            scratch_shapes=[
                pltpu.VMEM((span, LANES), jnp.bfloat16),
                pltpu.VMEM((span, 2 * LANES), jnp.bfloat16),
                pltpu.VMEM((heads_pair, block_q, LANES), jnp.float32),
                pltpu.VMEM((heads_pair, block_q, 2 * LANES), jnp.float32),
            ],
        ),
        compiler_params=pltpu.CompilerParams(vmem_limit_bytes=VMEM_LIMIT),
        cost_estimate=pl.CostEstimate(
            flops=16 * tok * span * LANES, bytes_accessed=12 * tok * LANES, transcendentals=0
        ),
        name="attend_own" if own else "attend_rest",
    )(
        *bounds, pick, query_rows, *[x[0] for x in blocks], *[x[2] for x in blocks],
        gates[:, pair * heads_pair : (pair + 1) * heads_pair], key_docs[None, :], docs[:, None],
        *(() if own else state),
    )


def send(x, axis, pairs):
    return lax.ppermute(x, axis, pairs)


def mix_kernel(info_ref, *refs, offsets, pairs):
    count = len(offsets)
    slabs, pieces = refs[: count * pairs], refs[count * pairs : count * (pairs + 1)]
    weight_ref, gain_ref, normed_ref, own_ref, hidden = refs[count * (pairs + 1) :]
    model = weight_ref.shape[1]
    width = weight_ref.shape[0] // count
    chunk = min(512, model)
    t = info_ref[0]
    j = pl.program_id(0)
    for i, offset in enumerate(offsets):

        @pl.when((t ^ j) == offset)
        def _(piece=pieces[i]):
            hidden[...] = piece[:, :model].astype(jnp.float32)

    heads = [
        jnp.concatenate([x[...] for x in slabs[i * pairs : (i + 1) * pairs]], axis=1)
        for i in range(count)
    ]
    squares = jnp.zeros((hidden.shape[0], LANES), jnp.float32)
    for c in range(0, model, chunk):
        total = hidden[:, c : c + chunk]
        for i in range(count):
            rows = pl.ds(pl.multiple_of((t ^ offsets[i]) * width, width), width)
            total = total + jnp.dot(
                heads[i], weight_ref[rows, c : c + chunk], preferred_element_type=jnp.float32
            )
        hidden[:, c : c + chunk] = total
        for l in range(0, chunk, LANES):
            squares = squares + total[:, l : l + LANES] * total[:, l : l + LANES]
    mean = jnp.sum(squares, axis=1, keepdims=True) * (1.0 / model)
    factor = lax.rsqrt(mean + norm_eps)
    for c in range(0, model, chunk):
        normed_ref[:, c : c + chunk] = (
            hidden[:, c : c + chunk] * factor * gain_ref[:, c : c + chunk]
        ).astype(normed_ref.dtype)

    @pl.when(t == j)
    def _():
        own_ref[...] = hidden[...]


def mix(t, offsets, pieces, rows, out_weight, norm_gain):
    tok_loc, wide_model = rows[0].shape
    model = out_weight.shape[1]
    parts = len(offsets)
    pairs = len(pieces[0])
    vmem = lambda shape: pl.BlockSpec(shape, lambda j, *_: (0, 0))
    return pl.pallas_call(
        functools.partial(mix_kernel, offsets=offsets, pairs=pairs),
        out_shape=[
            jax.ShapeDtypeStruct((parts * tok_loc, model), jnp.bfloat16),
            jax.ShapeDtypeStruct((tok_loc, model), jnp.float32),
        ],
        grid_spec=pltpu.PrefetchScalarGridSpec(
            num_scalar_prefetch=1,
            grid=(parts,),
            in_specs=[pl.BlockSpec((tok_loc, LANES), lambda j, *_: (j, 0))] * (parts * pairs)
            + [vmem((tok_loc, wide_model))] * parts
            + [vmem(out_weight.shape), vmem((1, model))],
            out_specs=[pl.BlockSpec((tok_loc, model), lambda j, *_: (j, 0)), vmem((tok_loc, model))],
            scratch_shapes=[pltpu.VMEM((tok_loc, model), jnp.float32)],
        ),
        compiler_params=pltpu.CompilerParams(vmem_limit_bytes=VMEM_LIMIT * 3 // 2),
        cost_estimate=pl.CostEstimate(
            flops=2 * parts * tok_loc * out_weight.size, bytes_accessed=16 << 20, transcendentals=0
        ),
        name="mix",
    )(
        t[None], *[y for x in pieces for y in x], *rows, out_weight, norm_gain[None],
    )


def act_block(x, parts_of, weight):
    depth = x.shape[1] // len(parts_of)
    product = jnp.dot(x[:, :depth], parts_of[0][...], preferred_element_type=jnp.float32)
    for i, part in enumerate(parts_of[1:], 1):
        product = product + jnp.dot(
            x[:, i * depth : (i + 1) * depth], part[...], preferred_element_type=jnp.float32
        )
    piece = product.shape[1] // 2
    gate, up = product[:, :piece], product[:, piece:]
    act = gate / (1.0 + jnp.exp(-gate)) * up
    return (act * weight).astype(jnp.bfloat16)


def acts_kernel(x_ref, weight_ref, *refs, first):
    out_ref = refs[-1]
    x = x_ref[...]
    out_ref[...] = jnp.concatenate(
        [
            act_block(x, [ref], weight_ref[:, first + i : first + i + 1])
            for i, ref in enumerate(refs[:-1])
        ],
        axis=1,
    )


def acts_of(normed, weights, first, shards):
    tok, model = normed.shape
    rows = min(256, tok)
    piece = shards[0].shape[1] // 2
    return pl.pallas_call(
        functools.partial(acts_kernel, first=first),
        out_shape=jax.ShapeDtypeStruct((tok, piece * len(shards)), jnp.bfloat16),
        grid=(tok // rows,),
        in_specs=[
            pl.BlockSpec((rows, model), lambda i: (i, 0)),
            pl.BlockSpec((rows, weights.shape[1]), lambda i: (i, 0)),
        ]
        + [pl.BlockSpec(x.shape, lambda i: (0, 0)) for x in shards],
        out_specs=pl.BlockSpec((rows, piece * len(shards)), lambda i: (i, 0)),
        compiler_params=pltpu.CompilerParams(vmem_limit_bytes=VMEM_LIMIT),
        cost_estimate=pl.CostEstimate(
            flops=4 * tok * model * piece * len(shards),
            bytes_accessed=2 * (normed.size + len(shards) * shards[0].size),
            transcendentals=0,
        ),
        name="acts",
    )(normed, weights, *shards)


def early_kernel(*refs, groups):
    acts, downs = refs[:groups], refs[groups:-2]
    out_ref, down_all = refs[-2:]
    piece = downs[0].shape[0]

    @pl.when(pl.program_id(0) == 0)
    def _():
        for i, x in enumerate(downs):
            down_all[pl.ds(i * piece, piece), :] = x[...]

    rows = jnp.concatenate([x[...] for x in acts], axis=1)
    chunk = min(512, out_ref.shape[1])
    for c in range(0, out_ref.shape[1], chunk):
        out_ref[:, c : c + chunk] = jnp.dot(
            rows, down_all[:, c : c + chunk], preferred_element_type=jnp.float32
        )


def early_sums(acts, downs):
    tok, (piece, model) = acts[0].shape[0], downs[0].shape
    rows = min(256, tok)
    return pl.pallas_call(
        functools.partial(early_kernel, groups=len(acts)),
        out_shape=jax.ShapeDtypeStruct((tok, model), jnp.float32),
        grid=(tok // rows,),
        in_specs=[pl.BlockSpec((rows, x.shape[1]), lambda i: (i, 0)) for x in acts]
        + [pl.BlockSpec(x.shape, lambda i: (0, 0)) for x in downs],
        out_specs=pl.BlockSpec((rows, model), lambda i: (i, 0)),
        scratch_shapes=[pltpu.VMEM((piece * len(downs), model), jnp.bfloat16)],
        compiler_params=pltpu.CompilerParams(vmem_limit_bytes=VMEM_LIMIT),
        cost_estimate=pl.CostEstimate(
            flops=2 * tok * piece * len(downs) * model, bytes_accessed=16 << 20, transcendentals=0
        ),
        name="early",
    )(*acts, *downs)


def last_kernel(block_ref, x_ref, weight_ref, early_ref, *refs, at, halves):
    wide, flat, out_ref = refs[:halves], refs[halves:-1], refs[-1]
    act = act_block(x_ref[...], wide, weight_ref[:, at : at + 1])
    lower = jnp.concatenate([x[...] for x in flat], axis=0)
    total = early_ref[...] + jnp.dot(act, lower, preferred_element_type=jnp.float32)
    out_ref[...] = total.astype(out_ref.dtype)


def last_sums(blocks, rows, normed, weights, at, early, wide, flat, dtype):
    model = normed.shape[1]
    pick = lambda g, block_ref: (block_ref[g], 0)
    whole = lambda x: pl.BlockSpec(x.shape, lambda g, *_: (0, 0))
    return pl.pallas_call(
        functools.partial(last_kernel, at=at, halves=len(wide)),
        out_shape=jax.ShapeDtypeStruct((blocks.shape[0] * rows, model), dtype),
        grid_spec=pltpu.PrefetchScalarGridSpec(
            num_scalar_prefetch=1,
            grid=(blocks.shape[0],),
            in_specs=[
                pl.BlockSpec((rows, model), pick),
                pl.BlockSpec((rows, weights.shape[1]), pick),
                pl.BlockSpec((rows, model), pick),
            ]
            + [whole(x) for x in (*wide, *flat)],
            out_specs=pl.BlockSpec((rows, model), lambda g, *_: (g, 0)),
        ),
        compiler_params=pltpu.CompilerParams(vmem_limit_bytes=VMEM_LIMIT),
        cost_estimate=pl.CostEstimate(
            flops=2 * blocks.shape[0] * rows * model * 384, bytes_accessed=8 << 20, transcendentals=0
        ),
        name="last",
    )(blocks, normed, weights, early, *wide, *flat)


def three_parts(x):
    high = lax.reduce_precision(x, 8, 7)
    middle = lax.reduce_precision(x - high, 8, 7)
    low = x - high - middle
    return [y.astype(jnp.bfloat16) for y in (high, middle, low)]


def per_device(
    query_rows, key_rows, value_rows, forget_cum, doc_ids, residual, out_weight, norm_gain,
    expert_ids, route_weights, gate_proj, up_proj, down_proj,
):
    n = lax.axis_size("sp")
    parts = lax.axis_size("tp")
    s = lax.axis_index("sp")
    t = lax.axis_index("tp")
    tok, width = query_rows.shape
    heads = forget_cum.shape[0]
    head_size = width // heads
    tok_loc, model = residual.shape
    hidden_units = gate_proj.shape[2]
    piece = hidden_units // parts

    after = lax.optimization_barrier
    flip = lambda bit: [(i, i ^ bit) for i in range(parts)]

    def behind(x):
        one = send(x, "sp", [(i, i + 1) for i in range(n - 1)])
        two = send(x, "sp", [(i, i + 2) for i in range(n - 2)])
        far = send(one, "sp", [(i, i + 2) for i in range(0, n - 2, 2)])
        side = send(two, "sp", [(i, i + 1) for i in range(0, n - 1, 2)])
        return side, far, two, one

    key_blocks = behind(key_rows)
    marks = jnp.concatenate([*three_parts(forget_cum), doc_ids[None].astype(jnp.bfloat16)])
    marks = jnp.pad(marks, ((0, 4 * heads - marks.shape[0]), (0, 0))).reshape(-1, width)
    value_blocks = behind(jnp.concatenate([value_rows, marks], axis=0))
    odd = s % 2 == 1

    def expert_at(place):
        place = (place + n) % n
        return jnp.where(place < (n + 1) // 2, 2 * place, 2 * (n - 1 - place) + 1)

    order = list(range(0, n, 2)) + list(range(1, n, 2))[::-1]
    forward = [(order[i], order[(i + 1) % n]) for i in range(n)]
    backward = [(b, a) for a, b in forward]
    place = jnp.where(s % 2 == 0, s // 2, n - 1 - s // 2)
    gate_up = jnp.concatenate(
        [
            lax.dynamic_slice_in_dim(gate_proj[0], t * piece, piece, 1),
            lax.dynamic_slice_in_dim(up_proj[0], t * piece, piece, 1),
        ],
        axis=1,
    )
    down = lax.dynamic_slice_in_dim(down_proj[0], t * piece, piece, 0)

    def ring(k, ahead, back):
        if 2 * k < n:
            return send(ahead, "sp", forward), send(back, "sp", backward)
        half = ahead.shape[0] // 2
        return send(ahead[:half], "sp", forward), send(back[half:], "sp", backward)

    steps = n // 2
    wide = {1: ring(1, gate_up, gate_up)}
    flat = {1: ring(1, down, down)}

    routes = jnp.concatenate([expert_ids.astype(jnp.bfloat16), *three_parts(route_weights)], axis=1)
    routes = jnp.pad(routes, ((0, 0), (0, LANES - routes.shape[1])))
    bits = [1 << b for b in range(parts.bit_length() - 1)]
    group = [(0, jnp.concatenate([residual, routes], axis=1))]
    for bit in bits[::-1]:
        group = group + [(o ^ bit, send(x, "tp", flip(bit))) for o, x in group]
    tail = jnp.zeros((tok, LANES), jnp.bfloat16)
    for o, x in group:
        tail = lax.dynamic_update_slice_in_dim(tail, x[:, model:], (t ^ o) * tok_loc, 0)
    topk = expert_ids.shape[1]
    tail = tail.astype(jnp.float32)
    group_ids = tail[:, :topk]
    group_weights = (
        tail[:, topk : 2 * topk] + tail[:, 2 * topk : 3 * topk] + tail[:, 3 * topk : 4 * topk]
    )
    places = [place] + [place + d for k in range(1, (n + 1) // 2) for d in (-k, k)]
    places += [place + n // 2] * (n % 2 == 0)
    arriving = jnp.stack([expert_at(x) for x in places]).astype(jnp.float32)
    weights = jnp.sum(
        jnp.where(group_ids[:, :, None] == arriving[None, None, :], group_weights[:, :, None], 0.0),
        axis=1,
    )

    nq = tok // min(BLOCK_Q, tok)
    pairs = width // LANES
    origin = forget_cum.reshape(heads, nq, tok // nq)[:, :, 0].T[:, :, None]
    docs = doc_ids.astype(jnp.float32)
    pick = jnp.where(odd, 0, 1).astype(jnp.int32)[None]
    own_bounds = visible(docs, docs)
    states = []
    for p in range(pairs):
        states.append(
            attend(
                p, query_rows, [(key_rows, 0, value_rows, 0)], (1,), pick, own_bounds,
                forget_cum[None] - origin, docs, docs, head_size, None,
            )
        )
    side, far, two, one = [x[tok:] for x in value_blocks]
    sent = [x.reshape(-1, tok).astype(jnp.float32) for x in (jnp.where(odd, side, far), two, one)]
    earlier = jnp.concatenate(
        [x[:heads] + x[heads : 2 * heads] + x[2 * heads : 3 * heads] for x in sent], axis=1
    )
    earlier_docs = jnp.concatenate(
        [jnp.where(REACH - i <= s, x[3 * heads], -1.0) for i, x in enumerate(sent)]
    )
    bounds = visible(earlier_docs, docs)
    relative = earlier[None] - origin
    attended = []
    for p in range(pairs):
        attended.append(
            attend(
                p, query_rows, [(x, 0, y, 0) for x, y in zip(key_blocks, value_blocks)],
                (2, 1, 1), pick, bounds, relative, earlier_docs, docs, head_size, states[p],
            )
        )
    wide[2] = ring(2, *wide[1])
    flat[2] = ring(2, *flat[1])

    pieces = [(0, tuple(attended))]
    for bit in bits[::-1]:
        pieces = pieces + [(o ^ bit, tuple(send(y, "tp", flip(bit)) for y in x)) for o, x in pieces]
    offsets = tuple(o for o, _ in pieces)
    normed, own_hidden = mix(
        t, offsets, [x for _, x in pieces], [x for _, x in group], out_weight, norm_gain
    )

    for k in range(3, steps + 1):
        wide[k] = ring(k, *wide[k - 1])
        flat[k] = ring(k, *flat[k - 1])
    acts, downs, first = [], [down], 0
    for k in range(1, steps):
        shards = [gate_up] * (k == 1) + list(wide[k])
        acts.append(acts_of(normed, weights, first, shards))
        first += len(shards)
        downs += list(flat[k])
    early = early_sums(acts, downs)

    def sums(offsets, dtype):
        blocks = jnp.stack([t ^ o for o in offsets]).astype(jnp.int32)
        return last_sums(
            blocks, tok_loc, normed, weights, first, early, wide[steps], flat[steps], dtype
        )

    keep = [0]
    for bit in bits[::-1][:-1]:
        keep = keep + [o ^ bit for o in keep]
    away = sums([o ^ bits[0] for o in keep], jnp.bfloat16)
    moved = send(away, "tp", flip(bits[0])).astype(jnp.float32)
    kept = sums(keep, jnp.float32)
    totals = {
        o: kept[i * tok_loc : (i + 1) * tok_loc] + moved[i * tok_loc : (i + 1) * tok_loc]
        for i, o in enumerate(keep)
    }
    totals[0] = totals[0] + own_hidden
    for bit in bits[1:]:
        for offset in [o for o in totals if o & bit]:
            moved = send(totals.pop(offset).astype(jnp.bfloat16), "tp", flip(bit))
            ready, moved = after((totals[offset ^ bit], moved))
            totals[offset ^ bit] = ready + moved.astype(jnp.float32)
    return totals[0].astype(jnp.bfloat16)


def solution(mesh):
    placed = (
        P("sp", "tp"),
        P("sp", "tp"),
        P("sp", "tp"),
        P("tp", "sp"),
        P("sp"),
        P(("sp", "tp"), None),
        P(),
        P(),
        P(("sp", "tp"), None),
        P(("sp", "tp"), None),
        P("sp", None, None),
        P("sp", None, None),
        P("sp", None, None),
    )
    return jax.shard_map(
        per_device, mesh=mesh, in_specs=placed, out_specs=P(("sp", "tp"), None), check_vma=False
    )
```

```python
import functools

import jax
import jax.numpy as jnp
from jax import lax
from jax.experimental import pallas as pl
from jax.experimental.pallas import tpu as pltpu
from jax.sharding import PartitionSpec as P


REACH = 3
LANES = 128
norm_eps = 1e-06
LOW = -1e30
VMEM_LIMIT = 32 * 1024 * 1024


def attend_kernel(
    low_ref, full_ref, pick_ref, q_ref, *refs, sources, own, heads_pair, block_k, scale,
):
    i = pl.program_id(0)
    block_q = q_ref.shape[0]
    count = sum(sources)
    k_refs, v_refs = refs[:count], refs[count : 2 * count]
    gate_ref, kdoc_ref, qdoc_ref = refs[2 * count : 2 * count + 3]
    state = refs[2 * count + 3 : -4]
    k_all, v_all, m_ref, acc_ref = refs[-4:]
    tok = k_refs[0].shape[0]
    head_size = LANES // heads_pair

    @pl.when(i == 0)
    def _():
        v_all[:, LANES:] = jnp.ones((v_all.shape[0], LANES), v_all.dtype)

        def fill(place, k_src, v_src):
            rows = pl.ds(place * tok, tok)
            k_all[rows, :] = k_src[...]
            v_all[rows, :LANES] = v_src[...]

        at = 0
        for place, options in enumerate(sources):
            if options == 1:
                fill(place, k_refs[at], v_refs[at])
            else:
                for o in range(options):
                    pl.when(pick_ref[0] == o)(
                        functools.partial(fill, place, k_refs[at + o], v_refs[at + o])
                    )
            at += options

    low, full = low_ref[i], full_ref[i]
    lane = lax.broadcasted_iota(jnp.int32, (block_q, LANES), 1)
    query = q_ref[...].astype(jnp.float32) * scale
    mine = [(lane // head_size) == h for h in range(heads_pair)]
    q_heads = [jnp.where(x, query, 0.0).astype(jnp.bfloat16) for x in mine]
    for h in range(heads_pair):
        if own:
            m_ref[h] = jnp.full((block_q, LANES), LOW, jnp.float32)
            acc_ref[h] = jnp.zeros((block_q, 2 * LANES), jnp.float32)
        else:
            m_ref[h] = jnp.broadcast_to(
                state[2][:, h * head_size : h * head_size + 1], (block_q, LANES)
            )
            acc_ref[h, :, :LANES] = state[0][...]
            acc_ref[h, :, LANES:] = state[1][...]

    def step(j, masked, causal):
        start = pl.multiple_of(j * block_k, block_k)
        rows = pl.ds(start, block_k)
        if masked:
            allowed = qdoc_ref[...] == kdoc_ref[:, rows]
            if causal:
                shape = (block_q, block_k)
                q_pos = i * block_q + lax.broadcasted_iota(jnp.int32, shape, 0)
                k_pos = start + lax.broadcasted_iota(jnp.int32, shape, 1)
                allowed = allowed & (k_pos <= q_pos)
        for h in range(heads_pair):
            score = lax.dot_general(
                q_heads[h], k_all[rows, :], (((1,), (1,)), ((), ())),
                preferred_element_type=jnp.float32,
            )
            score = score - gate_ref[0, h : h + 1, rows]
            if masked:
                score = jnp.where(allowed, score, LOW)
            before = m_ref[h]
            top = jnp.maximum(before, jnp.max(score, axis=1, keepdims=True))
            shrink = jnp.exp(before - top)
            m_ref[h] = top
            wide = jnp.concatenate([top] * (block_k // LANES), axis=1)
            expo = jnp.exp(score - wide).astype(jnp.bfloat16)
            product = jnp.dot(expo, v_all[rows, :], preferred_element_type=jnp.float32)
            acc_ref[h] = acc_ref[h] * jnp.concatenate([shrink, shrink], axis=1) + product

    def loop(first, end, masked, causal):
        def body(j, carry):
            step(j, masked, causal)
            return carry

        lax.fori_loop(first, end, body, 0)

    if own:
        loop(low, (i * block_q + block_q + block_k - 1) // block_k, True, True)
    else:
        loop(low, full, True, False)
        loop(full, len(sources) * tok // block_k, False, False)
    summed, total, top = (
        functools.reduce(
            lambda x, h: jnp.where(mine[h], parts[h], x), range(1, heads_pair), parts[0]
        )
        for parts in (
            [acc_ref[h, :, :LANES] for h in range(heads_pair)],
            [acc_ref[h, :, LANES:] for h in range(heads_pair)],
            [m_ref[h] for h in range(heads_pair)],
        )
    )
    if own:
        state[0][...] = summed
        state[1][...] = total
        state[2][...] = top
    else:
        state[3][...] = (summed / total).astype(state[3].dtype)


BLOCK_Q = 512
BLOCK_K = 512


def visible(key_docs, docs):
    block_q, block_k = min(BLOCK_Q, docs.shape[0]), min(BLOCK_K, docs.shape[0])
    blocked = key_docs.reshape(-1, block_k)
    query_docs = docs.reshape(-1, block_q)
    low = jnp.sum(blocked[None, :, -1] < query_docs[:, None, 0], axis=1).astype(jnp.int32)
    full = jnp.sum(blocked[None, :, 0] < query_docs[:, None, -1], axis=1).astype(jnp.int32)
    return low, full


def attend(pair, query_rows, blocks, sources, pick, bounds, gates, key_docs, docs, head_size, state):
    own = state is None
    tok = query_rows.shape[0]
    span = gates.shape[2]
    block_q, block_k = min(BLOCK_Q, tok), min(BLOCK_K, tok)
    nq = tok // block_q
    heads_pair = LANES // head_size
    slab = pl.BlockSpec((block_q, LANES), lambda i, *_: (i, 0))
    saved = jax.ShapeDtypeStruct((tok, LANES), jnp.float32)

    def column(at):
        return pl.BlockSpec((tok, LANES), lambda i, *_: (at, pair))

    return pl.pallas_call(
        functools.partial(
            attend_kernel,
            sources=sources,
            own=own,
            heads_pair=heads_pair,
            block_k=block_k,
            scale=head_size ** (-0.5),
        ),
        out_shape=[saved] * 3 if own else jax.ShapeDtypeStruct((tok, LANES), jnp.bfloat16),
        grid_spec=pltpu.PrefetchScalarGridSpec(
            num_scalar_prefetch=3,
            grid=(nq,),
            in_specs=[pl.BlockSpec((block_q, LANES), lambda i, *_: (i, pair))]
            + [column(x[1]) for x in blocks]
            + [column(x[3]) for x in blocks]
            + [
                pl.BlockSpec((1, heads_pair, span), lambda i, *_: (i, 0, 0)),
                pl.BlockSpec((1, span), lambda i, *_: (0, 0)),
                pl.BlockSpec((block_q, 1), lambda i, *_: (i, 0)),
            ]
            + ([] if own else [slab] * 3),
            out_specs=[slab] * 3 if own else slab,
            scratch_shapes=[
                pltpu.VMEM((span, LANES), jnp.bfloat16),
                pltpu.VMEM((span, 2 * LANES), jnp.bfloat16),
                pltpu.VMEM((heads_pair, block_q, LANES), jnp.float32),
                pltpu.VMEM((heads_pair, block_q, 2 * LANES), jnp.float32),
            ],
        ),
        compiler_params=pltpu.CompilerParams(vmem_limit_bytes=VMEM_LIMIT),
        cost_estimate=pl.CostEstimate(
            flops=16 * tok * span * LANES, bytes_accessed=12 * tok * LANES, transcendentals=0
        ),
        name="attend_own" if own else "attend_rest",
    )(
        *bounds, pick, query_rows, *[x[0] for x in blocks], *[x[2] for x in blocks],
        gates[:, pair * heads_pair : (pair + 1) * heads_pair], key_docs[None, :], docs[:, None],
        *(() if own else state),
    )


def send(x, axis, pairs):
    return lax.ppermute(x, axis, pairs)


def mix_kernel(info_ref, *refs, offsets, pairs):
    count = len(offsets)
    slabs, pieces = refs[: count * pairs], refs[count * pairs : count * (pairs + 1)]
    weight_ref, gain_ref, normed_ref, own_ref, hidden = refs[count * (pairs + 1) :]
    model = weight_ref.shape[1]
    width = weight_ref.shape[0] // count
    chunk = min(512, model)
    t = info_ref[0]
    j = pl.program_id(0)
    for i, offset in enumerate(offsets):

        @pl.when((t ^ j) == offset)
        def _(piece=pieces[i]):
            hidden[...] = piece[:, :model].astype(jnp.float32)

    heads = [
        jnp.concatenate([x[...] for x in slabs[i * pairs : (i + 1) * pairs]], axis=1)
        for i in range(count)
    ]
    squares = jnp.zeros((hidden.shape[0], LANES), jnp.float32)
    for c in range(0, model, chunk):
        total = hidden[:, c : c + chunk]
        for i in range(count):
            rows = pl.ds(pl.multiple_of((t ^ offsets[i]) * width, width), width)
            total = total + jnp.dot(
                heads[i], weight_ref[rows, c : c + chunk], preferred_element_type=jnp.float32
            )
        hidden[:, c : c + chunk] = total
        for l in range(0, chunk, LANES):
            squares = squares + total[:, l : l + LANES] * total[:, l : l + LANES]
    mean = jnp.sum(squares, axis=1, keepdims=True) * (1.0 / model)
    factor = lax.rsqrt(mean + norm_eps)
    for c in range(0, model, chunk):
        normed_ref[:, c : c + chunk] = (
            hidden[:, c : c + chunk] * factor * gain_ref[:, c : c + chunk]
        ).astype(normed_ref.dtype)

    @pl.when(t == j)
    def _():
        own_ref[...] = hidden[...]


def mix(t, offsets, pieces, rows, out_weight, norm_gain):
    tok_loc, wide_model = rows[0].shape
    model = out_weight.shape[1]
    parts = len(offsets)
    pairs = len(pieces[0])
    vmem = lambda shape: pl.BlockSpec(shape, lambda j, *_: (0, 0))
    return pl.pallas_call(
        functools.partial(mix_kernel, offsets=offsets, pairs=pairs),
        out_shape=[
            jax.ShapeDtypeStruct((parts * tok_loc, model), jnp.bfloat16),
            jax.ShapeDtypeStruct((tok_loc, model), jnp.float32),
        ],
        grid_spec=pltpu.PrefetchScalarGridSpec(
            num_scalar_prefetch=1,
            grid=(parts,),
            in_specs=[pl.BlockSpec((tok_loc, LANES), lambda j, *_: (j, 0))] * (parts * pairs)
            + [vmem((tok_loc, wide_model))] * parts
            + [vmem(out_weight.shape), vmem((1, model))],
            out_specs=[pl.BlockSpec((tok_loc, model), lambda j, *_: (j, 0)), vmem((tok_loc, model))],
            scratch_shapes=[pltpu.VMEM((tok_loc, model), jnp.float32)],
        ),
        compiler_params=pltpu.CompilerParams(vmem_limit_bytes=VMEM_LIMIT * 3 // 2),
        cost_estimate=pl.CostEstimate(
            flops=2 * parts * tok_loc * out_weight.size, bytes_accessed=16 << 20, transcendentals=0
        ),
        name="mix",
    )(
        t[None], *[y for x in pieces for y in x], *rows, out_weight, norm_gain[None],
    )


def act_block(x, parts_of, weight):
    depth = x.shape[1] // len(parts_of)
    product = jnp.dot(x[:, :depth], parts_of[0][...], preferred_element_type=jnp.float32)
    for i, part in enumerate(parts_of[1:], 1):
        product = product + jnp.dot(
            x[:, i * depth : (i + 1) * depth], part[...], preferred_element_type=jnp.float32
        )
    piece = product.shape[1] // 2
    gate, up = product[:, :piece], product[:, piece:]
    act = gate / (1.0 + jnp.exp(-gate)) * up
    return (act * weight).astype(jnp.bfloat16)


def acts_kernel(x_ref, weight_ref, *refs, first):
    out_ref = refs[-1]
    x = x_ref[...]
    out_ref[...] = jnp.concatenate(
        [
            act_block(x, [ref], weight_ref[:, first + i : first + i + 1])
            for i, ref in enumerate(refs[:-1])
        ],
        axis=1,
    )


def acts_of(normed, weights, first, shards):
    tok, model = normed.shape
    rows = min(256, tok)
    piece = shards[0].shape[1] // 2
    return pl.pallas_call(
        functools.partial(acts_kernel, first=first),
        out_shape=jax.ShapeDtypeStruct((tok, piece * len(shards)), jnp.bfloat16),
        grid=(tok // rows,),
        in_specs=[
            pl.BlockSpec((rows, model), lambda i: (i, 0)),
            pl.BlockSpec((rows, weights.shape[1]), lambda i: (i, 0)),
        ]
        + [pl.BlockSpec(x.shape, lambda i: (0, 0)) for x in shards],
        out_specs=pl.BlockSpec((rows, piece * len(shards)), lambda i: (i, 0)),
        compiler_params=pltpu.CompilerParams(vmem_limit_bytes=VMEM_LIMIT),
        cost_estimate=pl.CostEstimate(
            flops=4 * tok * model * piece * len(shards),
            bytes_accessed=2 * (normed.size + len(shards) * shards[0].size),
            transcendentals=0,
        ),
        name="acts",
    )(normed, weights, *shards)


def early_kernel(*refs, groups):
    acts, downs = refs[:groups], refs[groups:-2]
    out_ref, down_all = refs[-2:]
    piece = downs[0].shape[0]

    @pl.when(pl.program_id(0) == 0)
    def _():
        for i, x in enumerate(downs):
            down_all[pl.ds(i * piece, piece), :] = x[...]

    rows = jnp.concatenate([x[...] for x in acts], axis=1)
    chunk = min(512, out_ref.shape[1])
    for c in range(0, out_ref.shape[1], chunk):
        out_ref[:, c : c + chunk] = jnp.dot(
            rows, down_all[:, c : c + chunk], preferred_element_type=jnp.float32
        )


def early_sums(acts, downs):
    tok, (piece, model) = acts[0].shape[0], downs[0].shape
    rows = min(256, tok)
    return pl.pallas_call(
        functools.partial(early_kernel, groups=len(acts)),
        out_shape=jax.ShapeDtypeStruct((tok, model), jnp.float32),
        grid=(tok // rows,),
        in_specs=[pl.BlockSpec((rows, x.shape[1]), lambda i: (i, 0)) for x in acts]
        + [pl.BlockSpec(x.shape, lambda i: (0, 0)) for x in downs],
        out_specs=pl.BlockSpec((rows, model), lambda i: (i, 0)),
        scratch_shapes=[pltpu.VMEM((piece * len(downs), model), jnp.bfloat16)],
        compiler_params=pltpu.CompilerParams(vmem_limit_bytes=VMEM_LIMIT),
        cost_estimate=pl.CostEstimate(
            flops=2 * tok * piece * len(downs) * model, bytes_accessed=16 << 20, transcendentals=0
        ),
        name="early",
    )(*acts, *downs)


def last_kernel(block_ref, x_ref, weight_ref, early_ref, *refs, at, halves):
    wide, flat, out_ref = refs[:halves], refs[halves:-1], refs[-1]
    act = act_block(x_ref[...], wide, weight_ref[:, at : at + 1])
    lower = jnp.concatenate([x[...] for x in flat], axis=0)
    total = early_ref[...] + jnp.dot(act, lower, preferred_element_type=jnp.float32)
    out_ref[...] = total.astype(out_ref.dtype)


def last_sums(blocks, rows, normed, weights, at, early, wide, flat, dtype):
    model = normed.shape[1]
    pick = lambda g, block_ref: (block_ref[g], 0)
    whole = lambda x: pl.BlockSpec(x.shape, lambda g, *_: (0, 0))
    return pl.pallas_call(
        functools.partial(last_kernel, at=at, halves=len(wide)),
        out_shape=jax.ShapeDtypeStruct((blocks.shape[0] * rows, model), dtype),
        grid_spec=pltpu.PrefetchScalarGridSpec(
            num_scalar_prefetch=1,
            grid=(blocks.shape[0],),
            in_specs=[
                pl.BlockSpec((rows, model), pick),
                pl.BlockSpec((rows, weights.shape[1]), pick),
                pl.BlockSpec((rows, model), pick),
            ]
            + [whole(x) for x in (*wide, *flat)],
            out_specs=pl.BlockSpec((rows, model), lambda g, *_: (g, 0)),
        ),
        compiler_params=pltpu.CompilerParams(vmem_limit_bytes=VMEM_LIMIT),
        cost_estimate=pl.CostEstimate(
            flops=2 * blocks.shape[0] * rows * model * 384, bytes_accessed=8 << 20, transcendentals=0
        ),
        name="last",
    )(blocks, normed, weights, early, *wide, *flat)


def three_parts(x):
    high = lax.reduce_precision(x, 8, 7)
    middle = lax.reduce_precision(x - high, 8, 7)
    low = x - high - middle
    return [y.astype(jnp.bfloat16) for y in (high, middle, low)]


def per_device(
    query_rows, key_rows, value_rows, forget_cum, doc_ids, residual, out_weight, norm_gain,
    expert_ids, route_weights, gate_proj, up_proj, down_proj,
):
    n = lax.axis_size("sp")
    parts = lax.axis_size("tp")
    s = lax.axis_index("sp")
    t = lax.axis_index("tp")
    tok, width = query_rows.shape
    heads = forget_cum.shape[0]
    head_size = width // heads
    tok_loc, model = residual.shape
    hidden_units = gate_proj.shape[2]
    piece = hidden_units // parts

    after = lax.optimization_barrier
    flip = lambda bit: [(i, i ^ bit) for i in range(parts)]

    def behind(x):
        one = send(x, "sp", [(i, i + 1) for i in range(n - 1)])
        two = send(x, "sp", [(i, i + 2) for i in range(n - 2)])
        far = send(one, "sp", [(i, i + 2) for i in range(0, n - 2, 2)])
        side = send(two, "sp", [(i, i + 1) for i in range(0, n - 1, 2)])
        return side, far, two, one

    key_blocks = behind(key_rows)
    marks = jnp.concatenate([*three_parts(forget_cum), doc_ids[None].astype(jnp.bfloat16)])
    marks = jnp.pad(marks, ((0, 4 * heads - marks.shape[0]), (0, 0))).reshape(-1, width)
    value_blocks = behind(jnp.concatenate([value_rows, marks], axis=0))
    odd = s % 2 == 1

    def expert_at(place):
        place = (place + n) % n
        return jnp.where(place < (n + 1) // 2, 2 * place, 2 * (n - 1 - place) + 1)

    order = list(range(0, n, 2)) + list(range(1, n, 2))[::-1]
    forward = [(order[i], order[(i + 1) % n]) for i in range(n)]
    backward = [(b, a) for a, b in forward]
    place = jnp.where(s % 2 == 0, s // 2, n - 1 - s // 2)
    gate_up = jnp.concatenate(
        [
            lax.dynamic_slice_in_dim(gate_proj[0], t * piece, piece, 1),
            lax.dynamic_slice_in_dim(up_proj[0], t * piece, piece, 1),
        ],
        axis=1,
    )
    down = lax.dynamic_slice_in_dim(down_proj[0], t * piece, piece, 0)

    def ring(k, ahead, back):
        if 2 * k < n:
            return send(ahead, "sp", forward), send(back, "sp", backward)
        half = ahead.shape[0] // 2
        return send(ahead[:half], "sp", forward), send(back[half:], "sp", backward)

    steps = n // 2
    wide = {1: ring(1, gate_up, gate_up)}
    flat = {1: ring(1, down, down)}

    routes = jnp.concatenate([expert_ids.astype(jnp.bfloat16), *three_parts(route_weights)], axis=1)
    routes = jnp.pad(routes, ((0, 0), (0, LANES - routes.shape[1])))
    bits = [1 << b for b in range(parts.bit_length() - 1)]
    group = [(0, jnp.concatenate([residual, routes], axis=1))]
    for bit in bits[::-1]:
        group = group + [(o ^ bit, send(x, "tp", flip(bit))) for o, x in group]
    tail = jnp.zeros((tok, LANES), jnp.bfloat16)
    for o, x in group:
        tail = lax.dynamic_update_slice_in_dim(tail, x[:, model:], (t ^ o) * tok_loc, 0)
    topk = expert_ids.shape[1]
    tail = tail.astype(jnp.float32)
    group_ids = tail[:, :topk]
    group_weights = (
        tail[:, topk : 2 * topk] + tail[:, 2 * topk : 3 * topk] + tail[:, 3 * topk : 4 * topk]
    )
    places = [place] + [place + d for k in range(1, (n + 1) // 2) for d in (-k, k)]
    places += [place + n // 2] * (n % 2 == 0)
    arriving = jnp.stack([expert_at(x) for x in places]).astype(jnp.float32)
    weights = jnp.sum(
        jnp.where(group_ids[:, :, None] == arriving[None, None, :], group_weights[:, :, None], 0.0),
        axis=1,
    )

    nq = tok // min(BLOCK_Q, tok)
    pairs = width // LANES
    origin = forget_cum.reshape(heads, nq, tok // nq)[:, :, 0].T[:, :, None]
    docs = doc_ids.astype(jnp.float32)
    pick = jnp.where(odd, 0, 1).astype(jnp.int32)[None]
    own_bounds = visible(docs, docs)
    states = []
    for p in range(pairs):
        states.append(
            attend(
                p, query_rows, [(key_rows, 0, value_rows, 0)], (1,), pick, own_bounds,
                forget_cum[None] - origin, docs, docs, head_size, None,
            )
        )
    side, far, two, one = [x[tok:] for x in value_blocks]
    sent = [x.reshape(-1, tok).astype(jnp.float32) for x in (jnp.where(odd, side, far), two, one)]
    earlier = jnp.concatenate(
        [x[:heads] + x[heads : 2 * heads] + x[2 * heads : 3 * heads] for x in sent], axis=1
    )
    earlier_docs = jnp.concatenate(
        [jnp.where(REACH - i <= s, x[3 * heads], -1.0) for i, x in enumerate(sent)]
    )
    bounds = visible(earlier_docs, docs)
    relative = earlier[None] - origin
    attended = []
    for p in range(pairs):
        attended.append(
            attend(
                p, query_rows, [(x, 0, y, 0) for x, y in zip(key_blocks, value_blocks)],
                (2, 1, 1), pick, bounds, relative, earlier_docs, docs, head_size, states[p],
            )
        )
    wide[2] = ring(2, *wide[1])
    flat[2] = ring(2, *flat[1])

    pieces = [(0, tuple(attended))]
    for bit in bits[::-1]:
        pieces = pieces + [(o ^ bit, tuple(send(y, "tp", flip(bit)) for y in x)) for o, x in pieces]
    offsets = tuple(o for o, _ in pieces)
    normed, own_hidden = mix(
        t, offsets, [x for _, x in pieces], [x for _, x in group], out_weight, norm_gain
    )

    for k in range(3, steps + 1):
        wide[k] = ring(k, *wide[k - 1])
        flat[k] = ring(k, *flat[k - 1])
    acts, downs, first = [], [down], 0
    for k in range(1, steps):
        shards = [gate_up] * (k == 1) + list(wide[k])
        acts.append(acts_of(normed, weights, first, shards))
        first += len(shards)
        downs += list(flat[k])
    early = early_sums(acts, downs)

    def sums(offsets, dtype):
        blocks = jnp.stack([t ^ o for o in offsets]).astype(jnp.int32)
        return last_sums(
            blocks, tok_loc, normed, weights, first, early, wide[steps], flat[steps], dtype
        )

    keep = [0]
    for bit in bits[::-1][:-1]:
        keep = keep + [o ^ bit for o in keep]
    totals = {}
    for chosen in (bits[1], 0):
        group = [o for o in keep if o & bits[1] == chosen]
        away = sums([o ^ bits[0] for o in group], jnp.bfloat16)
        moved = send(away, "tp", flip(bits[0])).astype(jnp.float32)
        kept = sums(group, jnp.float32)
        for i, o in enumerate(group):
            rows = slice(i * tok_loc, (i + 1) * tok_loc)
            totals[o] = kept[rows] + moved[rows]
    totals[0] = totals[0] + own_hidden
    for bit in bits[1:]:
        for offset in [o for o in totals if o & bit]:
            moved = send(totals.pop(offset).astype(jnp.bfloat16), "tp", flip(bit))
            ready, moved = after((totals[offset ^ bit], moved))
            totals[offset ^ bit] = ready + moved.astype(jnp.float32)
    return totals[0].astype(jnp.bfloat16)


def solution(mesh):
    placed = (
        P("sp", "tp"),
        P("sp", "tp"),
        P("sp", "tp"),
        P("tp", "sp"),
        P("sp"),
        P(("sp", "tp"), None),
        P(),
        P(),
        P(("sp", "tp"), None),
        P(("sp", "tp"), None),
        P("sp", None, None),
        P("sp", None, None),
        P("sp", None, None),
    )
    return jax.shard_map(
        per_device, mesh=mesh, in_specs=placed, out_specs=P(("sp", "tp"), None), check_vma=False
    )
```

```python
import functools

import jax
import jax.numpy as jnp
from jax import lax
from jax.experimental import pallas as pl
from jax.experimental.pallas import tpu as pltpu
from jax.sharding import PartitionSpec as P


REACH = 3
LANES = 128
norm_eps = 1e-06
LOW = -1e30
VMEM_LIMIT = 32 * 1024 * 1024


def attend_kernel(
    low_ref, full_ref, pick_ref, q_ref, *refs, sources, own, heads_pair, block_k, scale,
):
    i = pl.program_id(0)
    block_q = q_ref.shape[0]
    count = sum(sources)
    k_refs, v_refs = refs[:count], refs[count : 2 * count]
    gate_ref, kdoc_ref, qdoc_ref = refs[2 * count : 2 * count + 3]
    state = refs[2 * count + 3 : -4]
    k_all, v_all, m_ref, acc_ref = refs[-4:]
    tok = k_refs[0].shape[0]
    head_size = LANES // heads_pair

    @pl.when(i == 0)
    def _():
        v_all[:, LANES:] = jnp.ones((v_all.shape[0], LANES), v_all.dtype)

        def fill(place, k_src, v_src):
            rows = pl.ds(place * tok, tok)
            k_all[rows, :] = k_src[...]
            v_all[rows, :LANES] = v_src[...]

        at = 0
        for place, options in enumerate(sources):
            if options == 1:
                fill(place, k_refs[at], v_refs[at])
            else:
                for o in range(options):
                    pl.when(pick_ref[0] == o)(
                        functools.partial(fill, place, k_refs[at + o], v_refs[at + o])
                    )
            at += options

    low, full = low_ref[i], full_ref[i]
    lane = lax.broadcasted_iota(jnp.int32, (block_q, LANES), 1)
    query = q_ref[...].astype(jnp.float32) * scale
    mine = [(lane // head_size) == h for h in range(heads_pair)]
    q_heads = [jnp.where(x, query, 0.0).astype(jnp.bfloat16) for x in mine]
    for h in range(heads_pair):
        if own:
            m_ref[h] = jnp.full((block_q, LANES), LOW, jnp.float32)
            acc_ref[h] = jnp.zeros((block_q, 2 * LANES), jnp.float32)
        else:
            m_ref[h] = jnp.broadcast_to(
                state[2][:, h * head_size : h * head_size + 1], (block_q, LANES)
            )
            acc_ref[h, :, :LANES] = state[0][...]
            acc_ref[h, :, LANES:] = state[1][...]

    def step(j, masked, causal):
        start = pl.multiple_of(j * block_k, block_k)
        rows = pl.ds(start, block_k)
        if masked:
            allowed = qdoc_ref[...] == kdoc_ref[:, rows]
            if causal:
                shape = (block_q, block_k)
                q_pos = i * block_q + lax.broadcasted_iota(jnp.int32, shape, 0)
                k_pos = start + lax.broadcasted_iota(jnp.int32, shape, 1)
                allowed = allowed & (k_pos <= q_pos)
        for h in range(heads_pair):
            score = lax.dot_general(
                q_heads[h], k_all[rows, :], (((1,), (1,)), ((), ())),
                preferred_element_type=jnp.float32,
            )
            score = score - gate_ref[0, h : h + 1, rows]
            if masked:
                score = jnp.where(allowed, score, LOW)
            before = m_ref[h]
            top = jnp.maximum(before, jnp.max(score, axis=1, keepdims=True))
            shrink = jnp.exp(before - top)
            m_ref[h] = top
            wide = jnp.concatenate([top] * (block_k // LANES), axis=1)
            expo = jnp.exp(score - wide).astype(jnp.bfloat16)
            product = jnp.dot(expo, v_all[rows, :], preferred_element_type=jnp.float32)
            acc_ref[h] = acc_ref[h] * jnp.concatenate([shrink, shrink], axis=1) + product

    def loop(first, end, masked, causal):
        def body(j, carry):
            step(j, masked, causal)
            return carry

        lax.fori_loop(first, end, body, 0)

    if own:
        loop(low, (i * block_q + block_q + block_k - 1) // block_k, True, True)
    else:
        loop(low, full, True, False)
        loop(full, len(sources) * tok // block_k, False, False)
    summed, total, top = (
        functools.reduce(
            lambda x, h: jnp.where(mine[h], parts[h], x), range(1, heads_pair), parts[0]
        )
        for parts in (
            [acc_ref[h, :, :LANES] for h in range(heads_pair)],
            [acc_ref[h, :, LANES:] for h in range(heads_pair)],
            [m_ref[h] for h in range(heads_pair)],
        )
    )
    if own:
        state[0][...] = summed
        state[1][...] = total
        state[2][...] = top
    else:
        state[3][...] = (summed / total).astype(state[3].dtype)


BLOCK_Q = 512
BLOCK_K = 512


def visible(key_docs, docs):
    block_q, block_k = min(BLOCK_Q, docs.shape[0]), min(BLOCK_K, docs.shape[0])
    blocked = key_docs.reshape(-1, block_k)
    query_docs = docs.reshape(-1, block_q)
    low = jnp.sum(blocked[None, :, -1] < query_docs[:, None, 0], axis=1).astype(jnp.int32)
    full = jnp.sum(blocked[None, :, 0] < query_docs[:, None, -1], axis=1).astype(jnp.int32)
    return low, full


def attend(pair, query_rows, blocks, sources, pick, bounds, gates, key_docs, docs, head_size, state):
    own = state is None
    tok = query_rows.shape[0]
    span = gates.shape[2]
    block_q, block_k = min(BLOCK_Q, tok), min(BLOCK_K, tok)
    nq = tok // block_q
    heads_pair = LANES // head_size
    slab = pl.BlockSpec((block_q, LANES), lambda i, *_: (i, 0))
    saved = jax.ShapeDtypeStruct((tok, LANES), jnp.float32)

    def column(at):
        return pl.BlockSpec((tok, LANES), lambda i, *_: (at, pair))

    return pl.pallas_call(
        functools.partial(
            attend_kernel,
            sources=sources,
            own=own,
            heads_pair=heads_pair,
            block_k=block_k,
            scale=head_size ** (-0.5),
        ),
        out_shape=[saved] * 3 if own else jax.ShapeDtypeStruct((tok, LANES), jnp.bfloat16),
        grid_spec=pltpu.PrefetchScalarGridSpec(
            num_scalar_prefetch=3,
            grid=(nq,),
            in_specs=[pl.BlockSpec((block_q, LANES), lambda i, *_: (i, pair))]
            + [column(x[1]) for x in blocks]
            + [column(x[3]) for x in blocks]
            + [
                pl.BlockSpec((1, heads_pair, span), lambda i, *_: (i, 0, 0)),
                pl.BlockSpec((1, span), lambda i, *_: (0, 0)),
                pl.BlockSpec((block_q, 1), lambda i, *_: (i, 0)),
            ]
            + ([] if own else [slab] * 3),
            out_specs=[slab] * 3 if own else slab,
            scratch_shapes=[
                pltpu.VMEM((span, LANES), jnp.bfloat16),
                pltpu.VMEM((span, 2 * LANES), jnp.bfloat16),
                pltpu.VMEM((heads_pair, block_q, LANES), jnp.float32),
                pltpu.VMEM((heads_pair, block_q, 2 * LANES), jnp.float32),
            ],
        ),
        compiler_params=pltpu.CompilerParams(vmem_limit_bytes=VMEM_LIMIT),
        cost_estimate=pl.CostEstimate(
            flops=16 * tok * span * LANES, bytes_accessed=12 * tok * LANES, transcendentals=0
        ),
        name="attend_own" if own else "attend_rest",
    )(
        *bounds, pick, query_rows, *[x[0] for x in blocks], *[x[2] for x in blocks],
        gates[:, pair * heads_pair : (pair + 1) * heads_pair], key_docs[None, :], docs[:, None],
        *(() if own else state),
    )


def send(x, axis, pairs):
    return lax.ppermute(x, axis, pairs)


def mix_kernel(info_ref, *refs, offsets, pairs):
    count = len(offsets)
    slabs, pieces = refs[: count * pairs], refs[count * pairs : count * (pairs + 1)]
    weight_ref, gain_ref, normed_ref, own_ref, hidden = refs[count * (pairs + 1) :]
    model = weight_ref.shape[1]
    width = weight_ref.shape[0] // count
    chunk = min(512, model)
    t = info_ref[0]
    j = pl.program_id(0)
    for i, offset in enumerate(offsets):

        @pl.when((t ^ j) == offset)
        def _(piece=pieces[i]):
            hidden[...] = piece[:, :model].astype(jnp.float32)

    heads = [
        jnp.concatenate([x[...] for x in slabs[i * pairs : (i + 1) * pairs]], axis=1)
        for i in range(count)
    ]
    squares = jnp.zeros((hidden.shape[0], LANES), jnp.float32)
    for c in range(0, model, chunk):
        total = hidden[:, c : c + chunk]
        for i in range(count):
            rows = pl.ds(pl.multiple_of((t ^ offsets[i]) * width, width), width)
            total = total + jnp.dot(
                heads[i], weight_ref[rows, c : c + chunk], preferred_element_type=jnp.float32
            )
        hidden[:, c : c + chunk] = total
        for l in range(0, chunk, LANES):
            squares = squares + total[:, l : l + LANES] * total[:, l : l + LANES]
    mean = jnp.sum(squares, axis=1, keepdims=True) * (1.0 / model)
    factor = lax.rsqrt(mean + norm_eps)
    for c in range(0, model, chunk):
        normed_ref[:, c : c + chunk] = (
            hidden[:, c : c + chunk] * factor * gain_ref[:, c : c + chunk]
        ).astype(normed_ref.dtype)

    @pl.when(t == j)
    def _():
        own_ref[...] = hidden[...]


def mix(t, offsets, pieces, rows, out_weight, norm_gain):
    tok_loc, wide_model = rows[0].shape
    model = out_weight.shape[1]
    parts = len(offsets)
    pairs = len(pieces[0])
    vmem = lambda shape: pl.BlockSpec(shape, lambda j, *_: (0, 0))
    return pl.pallas_call(
        functools.partial(mix_kernel, offsets=offsets, pairs=pairs),
        out_shape=[
            jax.ShapeDtypeStruct((parts * tok_loc, model), jnp.bfloat16),
            jax.ShapeDtypeStruct((tok_loc, model), jnp.float32),
        ],
        grid_spec=pltpu.PrefetchScalarGridSpec(
            num_scalar_prefetch=1,
            grid=(parts,),
            in_specs=[pl.BlockSpec((tok_loc, LANES), lambda j, *_: (j, 0))] * (parts * pairs)
            + [vmem((tok_loc, wide_model))] * parts
            + [vmem(out_weight.shape), vmem((1, model))],
            out_specs=[pl.BlockSpec((tok_loc, model), lambda j, *_: (j, 0)), vmem((tok_loc, model))],
            scratch_shapes=[pltpu.VMEM((tok_loc, model), jnp.float32)],
        ),
        compiler_params=pltpu.CompilerParams(vmem_limit_bytes=VMEM_LIMIT * 3 // 2),
        cost_estimate=pl.CostEstimate(
            flops=2 * parts * tok_loc * out_weight.size, bytes_accessed=16 << 20, transcendentals=0
        ),
        name="mix",
    )(
        t[None], *[y for x in pieces for y in x], *rows, out_weight, norm_gain[None],
    )


def act_block(x, parts_of, weight):
    depth = x.shape[1] // len(parts_of)
    product = jnp.dot(x[:, :depth], parts_of[0][...], preferred_element_type=jnp.float32)
    for i, part in enumerate(parts_of[1:], 1):
        product = product + jnp.dot(
            x[:, i * depth : (i + 1) * depth], part[...], preferred_element_type=jnp.float32
        )
    piece = product.shape[1] // 2
    gate, up = product[:, :piece], product[:, piece:]
    act = gate / (1.0 + jnp.exp(-gate)) * up
    return (act * weight).astype(jnp.bfloat16)


def acts_kernel(x_ref, weight_ref, *refs, first):
    out_ref = refs[-1]
    x = x_ref[...]
    out_ref[...] = jnp.concatenate(
        [
            act_block(x, [ref], weight_ref[:, first + i : first + i + 1])
            for i, ref in enumerate(refs[:-1])
        ],
        axis=1,
    )


def acts_of(normed, weights, first, shards):
    tok, model = normed.shape
    rows = min(256, tok)
    piece = shards[0].shape[1] // 2
    return pl.pallas_call(
        functools.partial(acts_kernel, first=first),
        out_shape=jax.ShapeDtypeStruct((tok, piece * len(shards)), jnp.bfloat16),
        grid=(tok // rows,),
        in_specs=[
            pl.BlockSpec((rows, model), lambda i: (i, 0)),
            pl.BlockSpec((rows, weights.shape[1]), lambda i: (i, 0)),
        ]
        + [pl.BlockSpec(x.shape, lambda i: (0, 0)) for x in shards],
        out_specs=pl.BlockSpec((rows, piece * len(shards)), lambda i: (i, 0)),
        compiler_params=pltpu.CompilerParams(vmem_limit_bytes=VMEM_LIMIT),
        cost_estimate=pl.CostEstimate(
            flops=4 * tok * model * piece * len(shards),
            bytes_accessed=2 * (normed.size + len(shards) * shards[0].size),
            transcendentals=0,
        ),
        name="acts",
    )(normed, weights, *shards)


def early_kernel(*refs, groups):
    acts, downs = refs[:groups], refs[groups:-2]
    out_ref, down_all = refs[-2:]
    piece = downs[0].shape[0]

    @pl.when(pl.program_id(0) == 0)
    def _():
        for i, x in enumerate(downs):
            down_all[pl.ds(i * piece, piece), :] = x[...]

    rows = jnp.concatenate([x[...] for x in acts], axis=1)
    chunk = min(512, out_ref.shape[1])
    for c in range(0, out_ref.shape[1], chunk):
        out_ref[:, c : c + chunk] = jnp.dot(
            rows, down_all[:, c : c + chunk], preferred_element_type=jnp.float32
        )


def early_sums(acts, downs):
    tok, (piece, model) = acts[0].shape[0], downs[0].shape
    rows = min(256, tok)
    return pl.pallas_call(
        functools.partial(early_kernel, groups=len(acts)),
        out_shape=jax.ShapeDtypeStruct((tok, model), jnp.float32),
        grid=(tok // rows,),
        in_specs=[pl.BlockSpec((rows, x.shape[1]), lambda i: (i, 0)) for x in acts]
        + [pl.BlockSpec(x.shape, lambda i: (0, 0)) for x in downs],
        out_specs=pl.BlockSpec((rows, model), lambda i: (i, 0)),
        scratch_shapes=[pltpu.VMEM((piece * len(downs), model), jnp.bfloat16)],
        compiler_params=pltpu.CompilerParams(vmem_limit_bytes=VMEM_LIMIT),
        cost_estimate=pl.CostEstimate(
            flops=2 * tok * piece * len(downs) * model, bytes_accessed=16 << 20, transcendentals=0
        ),
        name="early",
    )(*acts, *downs)


def last_kernel(block_ref, x_ref, weight_ref, early_ref, *refs, at, halves):
    wide, flat, out_ref = refs[:halves], refs[halves:-1], refs[-1]
    act = act_block(x_ref[...], wide, weight_ref[:, at : at + 1])
    lower = jnp.concatenate([x[...] for x in flat], axis=0)
    total = early_ref[...] + jnp.dot(act, lower, preferred_element_type=jnp.float32)
    out_ref[...] = total.astype(out_ref.dtype)


def last_sums(blocks, rows, normed, weights, at, early, wide, flat, dtype):
    model = normed.shape[1]
    pick = lambda g, block_ref: (block_ref[g], 0)
    whole = lambda x: pl.BlockSpec(x.shape, lambda g, *_: (0, 0))
    return pl.pallas_call(
        functools.partial(last_kernel, at=at, halves=len(wide)),
        out_shape=jax.ShapeDtypeStruct((blocks.shape[0] * rows, model), dtype),
        grid_spec=pltpu.PrefetchScalarGridSpec(
            num_scalar_prefetch=1,
            grid=(blocks.shape[0],),
            in_specs=[
                pl.BlockSpec((rows, model), pick),
                pl.BlockSpec((rows, weights.shape[1]), pick),
                pl.BlockSpec((rows, model), pick),
            ]
            + [whole(x) for x in (*wide, *flat)],
            out_specs=pl.BlockSpec((rows, model), lambda g, *_: (g, 0)),
        ),
        compiler_params=pltpu.CompilerParams(vmem_limit_bytes=VMEM_LIMIT),
        cost_estimate=pl.CostEstimate(
            flops=2 * blocks.shape[0] * rows * model * 384, bytes_accessed=8 << 20, transcendentals=0
        ),
        name="last",
    )(blocks, normed, weights, early, *wide, *flat)


def three_parts(x):
    high = lax.reduce_precision(x, 8, 7)
    middle = lax.reduce_precision(x - high, 8, 7)
    low = x - high - middle
    return [y.astype(jnp.bfloat16) for y in (high, middle, low)]


def per_device(
    query_rows, key_rows, value_rows, forget_cum, doc_ids, residual, out_weight, norm_gain,
    expert_ids, route_weights, gate_proj, up_proj, down_proj,
):
    n = lax.axis_size("sp")
    parts = lax.axis_size("tp")
    s = lax.axis_index("sp")
    t = lax.axis_index("tp")
    tok, width = query_rows.shape
    heads = forget_cum.shape[0]
    head_size = width // heads
    tok_loc, model = residual.shape
    hidden_units = gate_proj.shape[2]
    piece = hidden_units // parts

    after = lax.optimization_barrier
    flip = lambda bit: [(i, i ^ bit) for i in range(parts)]

    def behind(x, by_even):
        two = send(x, "sp", [(i, i + 2) for i in range(n - 2)])
        one = send(x, "sp", [(i, i + 1) for i in range(0, n - 1, 2)])
        swap = send(two, "sp", [(i, i ^ 1) for i in range(n)])
        if by_even:
            far = send(swap, "sp", [(i, i + 2) for i in range(0, n - 2, 2)])
        else:
            far = send(two, "sp", [(i, i + 1) for i in range(1, n - 1, 2)])
        return swap, far, two, one

    key_blocks = behind(key_rows, True)
    marks = jnp.concatenate([*three_parts(forget_cum), doc_ids[None].astype(jnp.bfloat16)])
    marks = jnp.pad(marks, ((0, 4 * heads - marks.shape[0]), (0, 0))).reshape(-1, width)
    value_blocks = behind(jnp.concatenate([value_rows, marks], axis=0), False)
    odd = s % 2 == 1

    def expert_at(place):
        place = (place + n) % n
        return jnp.where(place < (n + 1) // 2, 2 * place, 2 * (n - 1 - place) + 1)

    order = list(range(0, n, 2)) + list(range(1, n, 2))[::-1]
    forward = [(order[i], order[(i + 1) % n]) for i in range(n)]
    backward = [(b, a) for a, b in forward]
    place = jnp.where(s % 2 == 0, s // 2, n - 1 - s // 2)
    gate_up = jnp.concatenate(
        [
            lax.dynamic_slice_in_dim(gate_proj[0], t * piece, piece, 1),
            lax.dynamic_slice_in_dim(up_proj[0], t * piece, piece, 1),
        ],
        axis=1,
    )
    down = lax.dynamic_slice_in_dim(down_proj[0], t * piece, piece, 0)

    def ring(k, ahead, back):
        if 2 * k < n:
            return send(ahead, "sp", forward), send(back, "sp", backward)
        half = ahead.shape[0] // 2
        return send(ahead[:half], "sp", forward), send(back[half:], "sp", backward)

    steps = n // 2
    wide = {1: ring(1, gate_up, gate_up)}
    flat = {1: ring(1, down, down)}

    routes = jnp.concatenate([expert_ids.astype(jnp.bfloat16), *three_parts(route_weights)], axis=1)
    routes = jnp.pad(routes, ((0, 0), (0, LANES - routes.shape[1])))
    bits = [1 << b for b in range(parts.bit_length() - 1)]
    group = [(0, jnp.concatenate([residual, routes], axis=1))]
    for bit in bits[::-1]:
        group = group + [(o ^ bit, send(x, "tp", flip(bit))) for o, x in group]
    tail = jnp.zeros((tok, LANES), jnp.bfloat16)
    for o, x in group:
        tail = lax.dynamic_update_slice_in_dim(tail, x[:, model:], (t ^ o) * tok_loc, 0)
    topk = expert_ids.shape[1]
    tail = tail.astype(jnp.float32)
    group_ids = tail[:, :topk]
    group_weights = (
        tail[:, topk : 2 * topk] + tail[:, 2 * topk : 3 * topk] + tail[:, 3 * topk : 4 * topk]
    )
    places = [place] + [place + d for k in range(1, (n + 1) // 2) for d in (-k, k)]
    places += [place + n // 2] * (n % 2 == 0)
    arriving = jnp.stack([expert_at(x) for x in places]).astype(jnp.float32)
    weights = jnp.sum(
        jnp.where(group_ids[:, :, None] == arriving[None, None, :], group_weights[:, :, None], 0.0),
        axis=1,
    )

    nq = tok // min(BLOCK_Q, tok)
    pairs = width // LANES
    origin = forget_cum.reshape(heads, nq, tok // nq)[:, :, 0].T[:, :, None]
    docs = doc_ids.astype(jnp.float32)
    pick = jnp.where(odd, 0, 1).astype(jnp.int32)[None]
    own_bounds = visible(docs, docs)
    states = []
    for p in range(pairs):
        states.append(
            attend(
                p, query_rows, [(key_rows, 0, value_rows, 0)], (1,), pick, own_bounds,
                forget_cum[None] - origin, docs, docs, head_size, None,
            )
        )
    swap, far, two, one = [x[tok:] for x in value_blocks]
    sent = [
        x.reshape(-1, tok).astype(jnp.float32)
        for x in (jnp.where(odd, swap, far), two, jnp.where(odd, one, swap))
    ]
    earlier = jnp.concatenate(
        [x[:heads] + x[heads : 2 * heads] + x[2 * heads : 3 * heads] for x in sent], axis=1
    )
    earlier_docs = jnp.concatenate(
        [jnp.where(REACH - i <= s, x[3 * heads], -1.0) for i, x in enumerate(sent)]
    )
    bounds = visible(earlier_docs, docs)
    relative = earlier[None] - origin
    attended = []
    for p in range(pairs):
        attended.append(
            attend(
                p, query_rows, [
                    (x, 0, y, 0)
                    for x, y in zip((*key_blocks, key_blocks[0]), (*value_blocks, value_blocks[0]))
                ],
                (2, 1, 2), pick, bounds, relative, earlier_docs, docs, head_size, states[p],
            )
        )
    wide[2] = ring(2, *wide[1])
    flat[2] = ring(2, *flat[1])

    pieces = [(0, tuple(attended))]
    for bit in bits[::-1]:
        pieces = pieces + [(o ^ bit, tuple(send(y, "tp", flip(bit)) for y in x)) for o, x in pieces]
    offsets = tuple(o for o, _ in pieces)
    normed, own_hidden = mix(
        t, offsets, [x for _, x in pieces], [x for _, x in group], out_weight, norm_gain
    )

    for k in range(3, steps + 1):
        wide[k] = ring(k, *wide[k - 1])
        flat[k] = ring(k, *flat[k - 1])
    acts, downs, first = [], [down], 0
    for k in range(1, steps):
        shards = [gate_up] * (k == 1) + list(wide[k])
        acts.append(acts_of(normed, weights, first, shards))
        first += len(shards)
        downs += list(flat[k])
    early = early_sums(acts, downs)

    def sums(offsets, dtype):
        blocks = jnp.stack([t ^ o for o in offsets]).astype(jnp.int32)
        return last_sums(
            blocks, tok_loc, normed, weights, first, early, wide[steps], flat[steps], dtype
        )

    keep = [0]
    for bit in bits[::-1][:-1]:
        keep = keep + [o ^ bit for o in keep]
    totals = {}
    for chosen in (bits[1], 0):
        group = [o for o in keep if o & bits[1] == chosen]
        away = sums([o ^ bits[0] for o in group], jnp.bfloat16)
        moved = send(away, "tp", flip(bits[0])).astype(jnp.float32)
        kept = sums(group, jnp.float32)
        for i, o in enumerate(group):
            rows = slice(i * tok_loc, (i + 1) * tok_loc)
            totals[o] = kept[rows] + moved[rows]
    totals[0] = totals[0] + own_hidden
    for bit in bits[1:]:
        for offset in [o for o in totals if o & bit]:
            moved = send(totals.pop(offset).astype(jnp.bfloat16), "tp", flip(bit))
            ready, moved = after((totals[offset ^ bit], moved))
            totals[offset ^ bit] = ready + moved.astype(jnp.float32)
    return totals[0].astype(jnp.bfloat16)


def solution(mesh):
    placed = (
        P("sp", "tp"),
        P("sp", "tp"),
        P("sp", "tp"),
        P("tp", "sp"),
        P("sp"),
        P(("sp", "tp"), None),
        P(),
        P(),
        P(("sp", "tp"), None),
        P(("sp", "tp"), None),
        P("sp", None, None),
        P("sp", None, None),
        P("sp", None, None),
    )
    return jax.shard_map(
        per_device, mesh=mesh, in_specs=placed, out_specs=P(("sp", "tp"), None), check_vma=False
    )
```

```python
import functools

import jax
import jax.numpy as jnp
from jax import lax
from jax.experimental import pallas as pl
from jax.experimental.pallas import tpu as pltpu
from jax.sharding import PartitionSpec as P


REACH = 3
LANES = 128
norm_eps = 1e-06
LOW = -1e30
VMEM_LIMIT = 32 * 1024 * 1024


def attend_kernel(
    low_ref, full_ref, pick_ref, q_ref, *refs, sources, own, heads_pair, block_k, scale,
):
    i = pl.program_id(0)
    block_q = q_ref.shape[0]
    count = sum(sources)
    k_refs, v_refs = refs[:count], refs[count : 2 * count]
    gate_ref, kdoc_ref, qdoc_ref = refs[2 * count : 2 * count + 3]
    state = refs[2 * count + 3 : -4]
    k_all, v_all, m_ref, acc_ref = refs[-4:]
    tok = k_refs[0].shape[0]
    head_size = LANES // heads_pair

    @pl.when(i == 0)
    def _():
        v_all[:, LANES:] = jnp.ones((v_all.shape[0], LANES), v_all.dtype)

        def fill(place, k_src, v_src):
            rows = pl.ds(place * tok, tok)
            k_all[rows, :] = k_src[...]
            v_all[rows, :LANES] = v_src[...]

        at = 0
        for place, options in enumerate(sources):
            if options == 1:
                fill(place, k_refs[at], v_refs[at])
            else:
                for o in range(options):
                    pl.when(pick_ref[0] == o)(
                        functools.partial(fill, place, k_refs[at + o], v_refs[at + o])
                    )
            at += options

    low, full = low_ref[i], full_ref[i]
    lane = lax.broadcasted_iota(jnp.int32, (block_q, LANES), 1)
    query = q_ref[...].astype(jnp.float32) * scale
    mine = [(lane // head_size) == h for h in range(heads_pair)]
    q_heads = [jnp.where(x, query, 0.0).astype(jnp.bfloat16) for x in mine]
    for h in range(heads_pair):
        if own:
            m_ref[h] = jnp.full((block_q, LANES), LOW, jnp.float32)
            acc_ref[h] = jnp.zeros((block_q, 2 * LANES), jnp.float32)
        else:
            m_ref[h] = jnp.broadcast_to(
                state[2][:, h * head_size : h * head_size + 1], (block_q, LANES)
            )
            acc_ref[h, :, :LANES] = state[0][...]
            acc_ref[h, :, LANES:] = state[1][...]

    def step(j, masked, causal):
        start = pl.multiple_of(j * block_k, block_k)
        rows = pl.ds(start, block_k)
        if masked:
            allowed = qdoc_ref[...] == kdoc_ref[:, rows]
            if causal:
                shape = (block_q, block_k)
                q_pos = i * block_q + lax.broadcasted_iota(jnp.int32, shape, 0)
                k_pos = start + lax.broadcasted_iota(jnp.int32, shape, 1)
                allowed = allowed & (k_pos <= q_pos)
        for h in range(heads_pair):
            score = lax.dot_general(
                q_heads[h], k_all[rows, :], (((1,), (1,)), ((), ())),
                preferred_element_type=jnp.float32,
            )
            score = score - gate_ref[0, h : h + 1, rows]
            if masked:
                score = jnp.where(allowed, score, LOW)
            before = m_ref[h]
            top = jnp.maximum(before, jnp.max(score, axis=1, keepdims=True))
            shrink = jnp.exp(before - top)
            m_ref[h] = top
            wide = jnp.concatenate([top] * (block_k // LANES), axis=1)
            expo = jnp.exp(score - wide).astype(jnp.bfloat16)
            product = jnp.dot(expo, v_all[rows, :], preferred_element_type=jnp.float32)
            acc_ref[h] = acc_ref[h] * jnp.concatenate([shrink, shrink], axis=1) + product

    def loop(first, end, masked, causal):
        def body(j, carry):
            step(j, masked, causal)
            return carry

        lax.fori_loop(first, end, body, 0)

    if own:
        loop(low, (i * block_q + block_q + block_k - 1) // block_k, True, True)
    else:
        loop(low, full, True, False)
        loop(full, len(sources) * tok // block_k, False, False)
    summed, total, top = (
        functools.reduce(
            lambda x, h: jnp.where(mine[h], parts[h], x), range(1, heads_pair), parts[0]
        )
        for parts in (
            [acc_ref[h, :, :LANES] for h in range(heads_pair)],
            [acc_ref[h, :, LANES:] for h in range(heads_pair)],
            [m_ref[h] for h in range(heads_pair)],
        )
    )
    if own:
        state[0][...] = summed
        state[1][...] = total
        state[2][...] = top
    else:
        state[3][...] = (summed / total).astype(state[3].dtype)


BLOCK_Q = 512
BLOCK_K = 512


def visible(key_docs, docs):
    block_q, block_k = min(BLOCK_Q, docs.shape[0]), min(BLOCK_K, docs.shape[0])
    blocked = key_docs.reshape(-1, block_k)
    query_docs = docs.reshape(-1, block_q)
    low = jnp.sum(blocked[None, :, -1] < query_docs[:, None, 0], axis=1).astype(jnp.int32)
    full = jnp.sum(blocked[None, :, 0] < query_docs[:, None, -1], axis=1).astype(jnp.int32)
    return low, full


def attend(pair, query_rows, blocks, sources, pick, bounds, gates, key_docs, docs, head_size, state):
    own = state is None
    tok = query_rows.shape[0]
    span = gates.shape[2]
    block_q, block_k = min(BLOCK_Q, tok), min(BLOCK_K, tok)
    nq = tok // block_q
    heads_pair = LANES // head_size
    slab = pl.BlockSpec((block_q, LANES), lambda i, *_: (i, 0))
    saved = jax.ShapeDtypeStruct((tok, LANES), jnp.float32)

    def column(at):
        return pl.BlockSpec((tok, LANES), lambda i, *_: (at, pair))

    return pl.pallas_call(
        functools.partial(
            attend_kernel,
            sources=sources,
            own=own,
            heads_pair=heads_pair,
            block_k=block_k,
            scale=head_size ** (-0.5),
        ),
        out_shape=[saved] * 3 if own else jax.ShapeDtypeStruct((tok, LANES), jnp.bfloat16),
        grid_spec=pltpu.PrefetchScalarGridSpec(
            num_scalar_prefetch=3,
            grid=(nq,),
            in_specs=[pl.BlockSpec((block_q, LANES), lambda i, *_: (i, pair))]
            + [column(x[1]) for x in blocks]
            + [column(x[3]) for x in blocks]
            + [
                pl.BlockSpec((1, heads_pair, span), lambda i, *_: (i, 0, 0)),
                pl.BlockSpec((1, span), lambda i, *_: (0, 0)),
                pl.BlockSpec((block_q, 1), lambda i, *_: (i, 0)),
            ]
            + ([] if own else [slab] * 3),
            out_specs=[slab] * 3 if own else slab,
            scratch_shapes=[
                pltpu.VMEM((span, LANES), jnp.bfloat16),
                pltpu.VMEM((span, 2 * LANES), jnp.bfloat16),
                pltpu.VMEM((heads_pair, block_q, LANES), jnp.float32),
                pltpu.VMEM((heads_pair, block_q, 2 * LANES), jnp.float32),
            ],
        ),
        compiler_params=pltpu.CompilerParams(vmem_limit_bytes=VMEM_LIMIT),
        cost_estimate=pl.CostEstimate(
            flops=16 * tok * span * LANES, bytes_accessed=12 * tok * LANES, transcendentals=0
        ),
        name="attend_own" if own else "attend_rest",
    )(
        *bounds, pick, query_rows, *[x[0] for x in blocks], *[x[2] for x in blocks],
        gates[:, pair * heads_pair : (pair + 1) * heads_pair], key_docs[None, :], docs[:, None],
        *(() if own else state),
    )


def send(x, axis, pairs):
    return lax.ppermute(x, axis, pairs)


def mix_kernel(info_ref, *refs, offsets, pairs):
    count = len(offsets)
    slabs, pieces = refs[: count * pairs], refs[count * pairs : count * (pairs + 1)]
    weight_ref, gain_ref, normed_ref, own_ref, hidden = refs[count * (pairs + 1) :]
    model = weight_ref.shape[1]
    width = weight_ref.shape[0] // count
    chunk = min(512, model)
    t = info_ref[0]
    j = pl.program_id(0)
    for i, offset in enumerate(offsets):

        @pl.when((t ^ j) == offset)
        def _(piece=pieces[i]):
            hidden[...] = piece[:, :model].astype(jnp.float32)

    heads = [
        jnp.concatenate([x[...] for x in slabs[i * pairs : (i + 1) * pairs]], axis=1)
        for i in range(count)
    ]
    squares = jnp.zeros((hidden.shape[0], LANES), jnp.float32)
    for c in range(0, model, chunk):
        total = hidden[:, c : c + chunk]
        for i in range(count):
            rows = pl.ds(pl.multiple_of((t ^ offsets[i]) * width, width), width)
            total = total + jnp.dot(
                heads[i], weight_ref[rows, c : c + chunk], preferred_element_type=jnp.float32
            )
        hidden[:, c : c + chunk] = total
        for l in range(0, chunk, LANES):
            squares = squares + total[:, l : l + LANES] * total[:, l : l + LANES]
    mean = jnp.sum(squares, axis=1, keepdims=True) * (1.0 / model)
    factor = lax.rsqrt(mean + norm_eps)
    for c in range(0, model, chunk):
        normed_ref[:, c : c + chunk] = (
            hidden[:, c : c + chunk] * factor * gain_ref[:, c : c + chunk]
        ).astype(normed_ref.dtype)

    @pl.when(t == j)
    def _():
        own_ref[...] = hidden[...]


def mix(t, offsets, pieces, rows, out_weight, norm_gain):
    tok_loc, wide_model = rows[0].shape
    model = out_weight.shape[1]
    parts = len(offsets)
    pairs = len(pieces[0])
    vmem = lambda shape: pl.BlockSpec(shape, lambda j, *_: (0, 0))
    return pl.pallas_call(
        functools.partial(mix_kernel, offsets=offsets, pairs=pairs),
        out_shape=[
            jax.ShapeDtypeStruct((parts * tok_loc, model), jnp.bfloat16),
            jax.ShapeDtypeStruct((tok_loc, model), jnp.float32),
        ],
        grid_spec=pltpu.PrefetchScalarGridSpec(
            num_scalar_prefetch=1,
            grid=(parts,),
            in_specs=[pl.BlockSpec((tok_loc, LANES), lambda j, *_: (j, 0))] * (parts * pairs)
            + [vmem((tok_loc, wide_model))] * parts
            + [vmem(out_weight.shape), vmem((1, model))],
            out_specs=[pl.BlockSpec((tok_loc, model), lambda j, *_: (j, 0)), vmem((tok_loc, model))],
            scratch_shapes=[pltpu.VMEM((tok_loc, model), jnp.float32)],
        ),
        compiler_params=pltpu.CompilerParams(vmem_limit_bytes=VMEM_LIMIT * 3 // 2),
        cost_estimate=pl.CostEstimate(
            flops=2 * parts * tok_loc * out_weight.size, bytes_accessed=16 << 20, transcendentals=0
        ),
        name="mix",
    )(
        t[None], *[y for x in pieces for y in x], *rows, out_weight, norm_gain[None],
    )


def act_block(x, parts_of, weight):
    depth = x.shape[1] // len(parts_of)
    product = jnp.dot(x[:, :depth], parts_of[0][...], preferred_element_type=jnp.float32)
    for i, part in enumerate(parts_of[1:], 1):
        product = product + jnp.dot(
            x[:, i * depth : (i + 1) * depth], part[...], preferred_element_type=jnp.float32
        )
    piece = product.shape[1] // 2
    gate, up = product[:, :piece], product[:, piece:]
    act = gate / (1.0 + jnp.exp(-gate)) * up
    return (act * weight).astype(jnp.bfloat16)


def acts_kernel(x_ref, weight_ref, *refs, first):
    out_ref = refs[-1]
    x = x_ref[...]
    out_ref[...] = jnp.concatenate(
        [
            act_block(x, [ref], weight_ref[:, first + i : first + i + 1])
            for i, ref in enumerate(refs[:-1])
        ],
        axis=1,
    )


def acts_of(normed, weights, first, shards):
    tok, model = normed.shape
    rows = min(256, tok)
    piece = shards[0].shape[1] // 2
    return pl.pallas_call(
        functools.partial(acts_kernel, first=first),
        out_shape=jax.ShapeDtypeStruct((tok, piece * len(shards)), jnp.bfloat16),
        grid=(tok // rows,),
        in_specs=[
            pl.BlockSpec((rows, model), lambda i: (i, 0)),
            pl.BlockSpec((rows, weights.shape[1]), lambda i: (i, 0)),
        ]
        + [pl.BlockSpec(x.shape, lambda i: (0, 0)) for x in shards],
        out_specs=pl.BlockSpec((rows, piece * len(shards)), lambda i: (i, 0)),
        compiler_params=pltpu.CompilerParams(vmem_limit_bytes=VMEM_LIMIT),
        cost_estimate=pl.CostEstimate(
            flops=4 * tok * model * piece * len(shards),
            bytes_accessed=2 * (normed.size + len(shards) * shards[0].size),
            transcendentals=0,
        ),
        name="acts",
    )(normed, weights, *shards)


def early_kernel(*refs, groups):
    acts, downs = refs[:groups], refs[groups:-2]
    out_ref, down_all = refs[-2:]
    piece = downs[0].shape[0]

    @pl.when(pl.program_id(0) == 0)
    def _():
        for i, x in enumerate(downs):
            down_all[pl.ds(i * piece, piece), :] = x[...]

    rows = jnp.concatenate([x[...] for x in acts], axis=1)
    chunk = min(512, out_ref.shape[1])
    for c in range(0, out_ref.shape[1], chunk):
        out_ref[:, c : c + chunk] = jnp.dot(
            rows, down_all[:, c : c + chunk], preferred_element_type=jnp.float32
        ).astype(out_ref.dtype)


def early_sums(acts, downs):
    tok, (piece, model) = acts[0].shape[0], downs[0].shape
    rows = min(256, tok)
    return pl.pallas_call(
        functools.partial(early_kernel, groups=len(acts)),
        out_shape=jax.ShapeDtypeStruct((tok, model), jnp.bfloat16),
        grid=(tok // rows,),
        in_specs=[pl.BlockSpec((rows, x.shape[1]), lambda i: (i, 0)) for x in acts]
        + [pl.BlockSpec(x.shape, lambda i: (0, 0)) for x in downs],
        out_specs=pl.BlockSpec((rows, model), lambda i: (i, 0)),
        scratch_shapes=[pltpu.VMEM((piece * len(downs), model), jnp.bfloat16)],
        compiler_params=pltpu.CompilerParams(vmem_limit_bytes=VMEM_LIMIT),
        cost_estimate=pl.CostEstimate(
            flops=2 * tok * piece * len(downs) * model, bytes_accessed=16 << 20, transcendentals=0
        ),
        name="early",
    )(*acts, *downs)


def last_kernel(block_ref, x_ref, weight_ref, early_ref, *refs, at, halves):
    wide, flat, out_ref = refs[:halves], refs[halves:-1], refs[-1]
    act = act_block(x_ref[...], wide, weight_ref[:, at : at + 1])
    lower = jnp.concatenate([x[...] for x in flat], axis=0)
    total = jnp.dot(act, lower, preferred_element_type=jnp.float32)
    total = total + early_ref[...].astype(jnp.float32)
    out_ref[...] = total.astype(out_ref.dtype)


def last_sums(blocks, rows, normed, weights, at, early, wide, flat, dtype):
    model = normed.shape[1]
    pick = lambda g, block_ref: (block_ref[g], 0)
    whole = lambda x: pl.BlockSpec(x.shape, lambda g, *_: (0, 0))
    return pl.pallas_call(
        functools.partial(last_kernel, at=at, halves=len(wide)),
        out_shape=jax.ShapeDtypeStruct((blocks.shape[0] * rows, model), dtype),
        grid_spec=pltpu.PrefetchScalarGridSpec(
            num_scalar_prefetch=1,
            grid=(blocks.shape[0],),
            in_specs=[
                pl.BlockSpec((rows, model), pick),
                pl.BlockSpec((rows, weights.shape[1]), pick),
                pl.BlockSpec((rows, model), pick),
            ]
            + [whole(x) for x in (*wide, *flat)],
            out_specs=pl.BlockSpec((rows, model), lambda g, *_: (g, 0)),
        ),
        compiler_params=pltpu.CompilerParams(vmem_limit_bytes=VMEM_LIMIT),
        cost_estimate=pl.CostEstimate(
            flops=2 * blocks.shape[0] * rows * model * 384, bytes_accessed=8 << 20, transcendentals=0
        ),
        name="last",
    )(blocks, normed, weights, early, *wide, *flat)


def three_parts(x):
    high = lax.reduce_precision(x, 8, 7)
    middle = lax.reduce_precision(x - high, 8, 7)
    low = x - high - middle
    return [y.astype(jnp.bfloat16) for y in (high, middle, low)]


def per_device(
    query_rows, key_rows, value_rows, forget_cum, doc_ids, residual, out_weight, norm_gain,
    expert_ids, route_weights, gate_proj, up_proj, down_proj,
):
    n = lax.axis_size("sp")
    parts = lax.axis_size("tp")
    s = lax.axis_index("sp")
    t = lax.axis_index("tp")
    tok, width = query_rows.shape
    heads = forget_cum.shape[0]
    head_size = width // heads
    tok_loc, model = residual.shape
    hidden_units = gate_proj.shape[2]
    piece = hidden_units // parts

    after = lax.optimization_barrier
    flip = lambda bit: [(i, i ^ bit) for i in range(parts)]

    def behind(x, by_even):
        two = send(x, "sp", [(i, i + 2) for i in range(n - 2)])
        one = send(x, "sp", [(i, i + 1) for i in range(0, n - 1, 2)])
        swap = send(two, "sp", [(i, i ^ 1) for i in range(n)])
        if by_even:
            far = send(swap, "sp", [(i, i + 2) for i in range(0, n - 2, 2)])
        else:
            far = send(two, "sp", [(i, i + 1) for i in range(1, n - 1, 2)])
        return swap, far, two, one

    key_blocks = behind(key_rows, True)
    marks = jnp.concatenate([*three_parts(forget_cum), doc_ids[None].astype(jnp.bfloat16)])
    marks = jnp.pad(marks, ((0, 4 * heads - marks.shape[0]), (0, 0))).reshape(-1, width)
    value_blocks = behind(jnp.concatenate([value_rows, marks], axis=0), False)
    odd = s % 2 == 1

    def expert_at(place):
        place = (place + n) % n
        return jnp.where(place < (n + 1) // 2, 2 * place, 2 * (n - 1 - place) + 1)

    order = list(range(0, n, 2)) + list(range(1, n, 2))[::-1]
    forward = [(order[i], order[(i + 1) % n]) for i in range(n)]
    backward = [(b, a) for a, b in forward]
    place = jnp.where(s % 2 == 0, s // 2, n - 1 - s // 2)
    gate_up = jnp.concatenate(
        [
            lax.dynamic_slice_in_dim(gate_proj[0], t * piece, piece, 1),
            lax.dynamic_slice_in_dim(up_proj[0], t * piece, piece, 1),
        ],
        axis=1,
    )
    down = lax.dynamic_slice_in_dim(down_proj[0], t * piece, piece, 0)

    def ring(k, ahead, back):
        if 2 * k < n:
            return send(ahead, "sp", forward), send(back, "sp", backward)
        half = ahead.shape[0] // 2
        return send(ahead[:half], "sp", forward), send(back[half:], "sp", backward)

    steps = n // 2
    wide = {1: ring(1, gate_up, gate_up)}
    flat = {1: ring(1, down, down)}

    routes = jnp.concatenate([expert_ids.astype(jnp.bfloat16), *three_parts(route_weights)], axis=1)
    routes = jnp.pad(routes, ((0, 0), (0, LANES - routes.shape[1])))
    bits = [1 << b for b in range(parts.bit_length() - 1)]
    group = [(0, jnp.concatenate([residual, routes], axis=1))]
    for bit in bits[::-1]:
        group = group + [(o ^ bit, send(x, "tp", flip(bit))) for o, x in group]
    tail = jnp.zeros((tok, LANES), jnp.bfloat16)
    for o, x in group:
        tail = lax.dynamic_update_slice_in_dim(tail, x[:, model:], (t ^ o) * tok_loc, 0)
    topk = expert_ids.shape[1]
    tail = tail.astype(jnp.float32)
    group_ids = tail[:, :topk]
    group_weights = (
        tail[:, topk : 2 * topk] + tail[:, 2 * topk : 3 * topk] + tail[:, 3 * topk : 4 * topk]
    )
    places = [place] + [place + d for k in range(1, (n + 1) // 2) for d in (-k, k)]
    places += [place + n // 2] * (n % 2 == 0)
    arriving = jnp.stack([expert_at(x) for x in places]).astype(jnp.float32)
    weights = jnp.sum(
        jnp.where(group_ids[:, :, None] == arriving[None, None, :], group_weights[:, :, None], 0.0),
        axis=1,
    )

    nq = tok // min(BLOCK_Q, tok)
    pairs = width // LANES
    origin = forget_cum.reshape(heads, nq, tok // nq)[:, :, 0].T[:, :, None]
    docs = doc_ids.astype(jnp.float32)
    pick = jnp.where(odd, 0, 1).astype(jnp.int32)[None]
    own_bounds = visible(docs, docs)
    states = []
    for p in range(pairs):
        states.append(
            attend(
                p, query_rows, [(key_rows, 0, value_rows, 0)], (1,), pick, own_bounds,
                forget_cum[None] - origin, docs, docs, head_size, None,
            )
        )
    swap, far, two, one = [x[tok:] for x in value_blocks]
    sent = [
        x.reshape(-1, tok).astype(jnp.float32)
        for x in (jnp.where(odd, swap, far), two, jnp.where(odd, one, swap))
    ]
    earlier = jnp.concatenate(
        [x[:heads] + x[heads : 2 * heads] + x[2 * heads : 3 * heads] for x in sent], axis=1
    )
    earlier_docs = jnp.concatenate(
        [jnp.where(REACH - i <= s, x[3 * heads], -1.0) for i, x in enumerate(sent)]
    )
    bounds = visible(earlier_docs, docs)
    relative = earlier[None] - origin
    attended = []
    for p in range(pairs):
        attended.append(
            attend(
                p, query_rows, [
                    (x, 0, y, 0)
                    for x, y in zip((*key_blocks, key_blocks[0]), (*value_blocks, value_blocks[0]))
                ],
                (2, 1, 2), pick, bounds, relative, earlier_docs, docs, head_size, states[p],
            )
        )
    wide[2] = ring(2, *wide[1])
    flat[2] = ring(2, *flat[1])

    pieces = [(0, tuple(attended))]
    for bit in bits[::-1]:
        pieces = pieces + [(o ^ bit, tuple(send(y, "tp", flip(bit)) for y in x)) for o, x in pieces]
    offsets = tuple(o for o, _ in pieces)
    normed, own_hidden = mix(
        t, offsets, [x for _, x in pieces], [x for _, x in group], out_weight, norm_gain
    )

    for k in range(3, steps + 1):
        wide[k] = ring(k, *wide[k - 1])
        flat[k] = ring(k, *flat[k - 1])
    acts, downs, first = [], [down], 0
    for k in range(1, steps):
        shards = [gate_up] * (k == 1) + list(wide[k])
        acts.append(acts_of(normed, weights, first, shards))
        first += len(shards)
        downs += list(flat[k])
    early = early_sums(acts, downs)

    def sums(offsets, dtype):
        blocks = jnp.stack([t ^ o for o in offsets]).astype(jnp.int32)
        return last_sums(
            blocks, tok_loc, normed, weights, first, early, wide[steps], flat[steps], dtype
        )

    keep = [0]
    for bit in bits[::-1][:-1]:
        keep = keep + [o ^ bit for o in keep]
    totals = {}
    for chosen in (bits[1], 0):
        group = [o for o in keep if o & bits[1] == chosen]
        away = sums([o ^ bits[0] for o in group], jnp.bfloat16)
        moved = send(away, "tp", flip(bits[0])).astype(jnp.float32)
        kept = sums(group, jnp.float32)
        for i, o in enumerate(group):
            rows = slice(i * tok_loc, (i + 1) * tok_loc)
            totals[o] = kept[rows] + moved[rows]
    totals[0] = totals[0] + own_hidden
    for bit in bits[1:]:
        for offset in [o for o in totals if o & bit]:
            moved = send(totals.pop(offset).astype(jnp.bfloat16), "tp", flip(bit))
            ready, moved = after((totals[offset ^ bit], moved))
            totals[offset ^ bit] = ready + moved.astype(jnp.float32)
    return totals[0].astype(jnp.bfloat16)


def solution(mesh):
    placed = (
        P("sp", "tp"),
        P("sp", "tp"),
        P("sp", "tp"),
        P("tp", "sp"),
        P("sp"),
        P(("sp", "tp"), None),
        P(),
        P(),
        P(("sp", "tp"), None),
        P(("sp", "tp"), None),
        P("sp", None, None),
        P("sp", None, None),
        P("sp", None, None),
    )
    return jax.shard_map(
        per_device, mesh=mesh, in_specs=placed, out_specs=P(("sp", "tp"), None), check_vma=False
    )
```
